256 devices in a mesh: tp: 32 (over z, y), dp: 8 (over x, core).
Axes of the slice: x: 4, y: 4, z: 8, core: 2. Of those that a mesh axis runs over, the one named last changes fastest.
Arguments:
- tokens: bfloat16 [192, 1024], P('tp', 'dp'), may hold values from -6 to 6
- lengths: int32 [192], P('dp'), may hold values from 1 to 8, 384 in all
- norm_gain: float32 [2, 1024], P(None, 'dp'), may hold values from 0.1 to 1.9
- w_gate: bfloat16 [2, 1024, 2048], P(None, 'dp', 'tp'), may hold values from -0.1875 to 0.1875
- w_value: bfloat16 [2, 1024, 2048], P(None, 'dp', 'tp'), may hold values from -0.1875 to 0.1875
- w_write: bfloat16 [2, 1024, 256], P(None, 'dp', 'tp'), may hold values from -0.1875 to 0.1875
- w_read: bfloat16 [2, 1024, 256], P(None, 'dp', 'tp'), may hold values from -0.1875 to 0.1875
- w_step: bfloat16 [2, 1024, 32], P(None, 'dp', 'tp'), may hold values from -0.1875 to 0.1875
- step_bias: float32 [2, 32], P(None, 'tp'), may hold values from -1 to 1
- decay_rate: float32 [2, 32], P(None, 'tp'), may hold values from 0.5 to 4
- skip_gain: float32 [2, 32], P(None, 'tp'), may hold values from 0.5 to 2
- conv_value_w: float32 [2, 4, 2048], P(None, None, 'tp'), may hold values from -3 to 3
- conv_write_w: float32 [2, 4, 256], P(None, None, 'tp'), may hold values from -3 to 3
- conv_read_w: float32 [2, 4, 256], P(None, None, 'tp'), may hold values from -3 to 3
- group_gain: float32 [2, 2048], P(None, 'tp'), may hold values from 0.1 to 1.9
- w_out: bfloat16 [2, 2048, 1024], P(None, 'tp', 'dp'), may hold values from -0.125 to 0.125
- state: float32 [2, 192, 32, 64, 128], P(None, 'dp', 'tp'), may hold values from -0.6 to 0.6
- hist_value: bfloat16 [2, 192, 3, 2048], P(None, 'dp', None, 'tp'), may hold values from -6 to 6
- hist_write: bfloat16 [2, 192, 3, 256], P(None, 'dp', None, 'tp'), may hold values from -6 to 6
- hist_read: bfloat16 [2, 192, 3, 256], P(None, 'dp', None, 'tp'), may hold values from -6 to 6
Outputs:
- mixed: float32 [192, 1024], P('tp', 'dp')
- new_state: float32 [2, 192, 32, 64, 128], P(None, 'dp', 'tp')
- new_hist_value: bfloat16 [2, 192, 3, 2048], P(None, 'dp', None, 'tp')
- new_hist_write: bfloat16 [2, 192, 3, 256], P(None, 'dp', None, 'tp')
- new_hist_read: bfloat16 [2, 192, 3, 256], P(None, 'dp', None, 'tp')
The draws below stay inside these ranges and needn't reach their ends.
Inputs may be any that keep to these rules, and one draw needn't show every extreme that they name: `lengths`: each sequence holds between 1 and 8 tokens before this step, and some sequence holds exactly 8.
All inputs are finite; a program needn't handle non-finite values.
Results may differ from the reference program's by a relative error of at most 0.03.
Values may be sent and summed in bfloat16 or wider, within the bound.
A program may use at most 64 MiB of HBM per device.

```python
import math
import jax
import jax.numpy as jnp
import numpy as np
from jax import lax

D = 1024
HEAD_DIM = 64
STATE = 128
GROUPS = 2
KERNEL = 4
HEADS = 32
WIDTH = 2048
SEQS = 192


def block_levels(own_key, dims, split, low, high):
    def one(position, blocks):
        draws = jax.random.uniform(jax.random.fold_in(jax.random.fold_in(own_key, 6), position), (blocks,), jnp.float32, low / len(split), high / len(split))
        return jnp.repeat(jnp.exp(draws), dims[position] // blocks).reshape((-1,) + (1,) * (len(dims) - position - 1))

    loudness = one(*split[0])
    for cut in split[1:]:
        loudness = loudness * one(*cut)
    return loudness


def profile(count, total, reach, lean):
    loads = [(1 << 20) // math.isqrt(rank ** lean) + 1 for rank in range(2, count + 1)]
    rest, given = total - reach - (count - 1), [1] * (count - 1)
    while rest > 0:
        free = [i for i in range(count - 1) if given[i] < reach]
        whole, left = sum([loads[i] for i in free]), rest
        for i in free:
            more = min(reach - given[i], max(1, left * loads[i] // whole), rest)
            given[i] = given[i] + more
            rest = rest - more
    return np.array([reach] + given)


def ragged(rng, number_of, total, limit, skew):
    if number_of == 2:
        one = jax.random.randint(rng, (), max(1, total - limit), min(limit, total - 1) + 1)
        return jnp.stack([one, total - one])
    tallies = jnp.asarray(profile(number_of, total, limit, skew), jnp.int32)
    pairs = (number_of - 1) // 2
    source_of, receiver = tallies[1:1 + 2 * pairs:2], tallies[2:2 + 2 * pairs:2]
    room = jnp.minimum(source_of - 1, limit - receiver)
    moved = jax.random.randint(jax.random.fold_in(rng, 1), (pairs,), 0, 1 << 20) % (room + 1)
    tallies = tallies.at[1:1 + 2 * pairs:2].set(source_of - moved).at[2:2 + 2 * pairs:2].set(receiver + moved)
    return tallies[jax.random.permutation(jax.random.fold_in(rng, 2), number_of)]


def noise(stream_key, dims, width, bound, cuts=(), kind=jnp.bfloat16):
    level = block_levels(stream_key, dims, cuts, -0.22, 0.18) if cuts else 1.0
    values = jax.random.normal(stream_key, dims, jnp.float32) * width * level
    return jnp.minimum(jnp.maximum(values, -bound), bound).astype(kind)


def setup_inputs(seed: int = 0) -> dict:
    key_list = jax.random.split(jax.random.key(seed), 21)
    tokens = noise(key_list[0], (SEQS, D), 1.0, 6.0, ((0, 32), (1, 8)))
    lengths = ragged(key_list[1], SEQS, 2 * SEQS, 8, 2).astype(jnp.int32)
    norm_gain = jnp.clip(1.0 + 0.18 * jax.random.normal(key_list[2], (2, D), jnp.float32), 0.1, 1.9)
    w_gate = noise(key_list[3], (2, D, WIDTH), D ** -0.5, 0.1875, ((1, 8), (2, 32)))
    w_value = noise(key_list[4], (2, D, WIDTH), D ** -0.5, 0.1875, ((1, 8), (2, 32)))
    w_write = noise(key_list[5], (2, D, GROUPS * STATE), D ** -0.5, 0.1875, ((1, 8), (2, 32)))
    w_read = noise(key_list[6], (2, D, GROUPS * STATE), D ** -0.5, 0.1875, ((1, 8), (2, 32)))
    w_step = noise(key_list[7], (2, D, HEADS), D ** -0.5, 0.1875, ((1, 8), (2, 32)))
    step_bias = jnp.clip(jax.random.uniform(key_list[8], (2, HEADS), jnp.float32, -1.0, 1.0) * block_levels(key_list[8], (2, HEADS), ((1, 32),), -0.4, 0.0), -1.0, 1.0)
    decay_rate = jnp.clip(jnp.exp(math.log(4.0) - 2.0794415 * jax.random.uniform(key_list[9], (2, HEADS), jnp.float32) ** block_levels(key_list[9], (2, HEADS), ((1, 32),), -0.2, 0.2)), 0.5, 4.0)
    skip_gain = jnp.clip(0.5 + 1.5 * jax.random.uniform(key_list[10], (2, HEADS), jnp.float32) ** block_levels(key_list[10], (2, HEADS), ((1, 32),), -0.2, 0.2), 0.5, 2.0)
    conv_value_w = noise(key_list[11], (2, KERNEL, WIDTH), KERNEL ** -0.5, 3.0, ((2, 32),), jnp.float32)
    conv_write_w = noise(key_list[12], (2, KERNEL, GROUPS * STATE), KERNEL ** -0.5, 3.0, ((2, 32),), jnp.float32)
    conv_read_w = noise(key_list[13], (2, KERNEL, GROUPS * STATE), KERNEL ** -0.5, 3.0, ((2, 32),), jnp.float32)
    group_gain = jnp.clip(1.0 + 0.18 * jax.random.normal(key_list[14], (2, WIDTH), jnp.float32), 0.1, 1.9)
    w_out = noise(key_list[15], (2, WIDTH, D), WIDTH ** -0.5, 0.125, ((1, 32), (2, 8)))
    state = noise(key_list[16], (2, SEQS, HEADS, HEAD_DIM, STATE), 0.1, 0.6, ((1, 8), (2, 32)), jnp.float32)
    hist_value = noise(key_list[17], (2, SEQS, KERNEL - 1, WIDTH), 1.0, 6.0, ((1, 8), (3, 32)))
    hist_write = noise(key_list[18], (2, SEQS, KERNEL - 1, GROUPS * STATE), 1.0, 6.0, ((1, 8), (3, 32)))
    hist_read = noise(key_list[19], (2, SEQS, KERNEL - 1, GROUPS * STATE), 1.0, 6.0, ((1, 8), (3, 32)))
    return {"tokens": tokens, "lengths": lengths, "norm_gain": norm_gain, "w_gate": w_gate, "w_value": w_value, "w_write": w_write, "w_read": w_read, "w_step": w_step, "step_bias": step_bias, "decay_rate": decay_rate, "skip_gain": skip_gain, "conv_value_w": conv_value_w, "conv_write_w": conv_write_w, "conv_read_w": conv_read_w, "group_gain": group_gain, "w_out": w_out, "state": state, "hist_value": hist_value, "hist_write": hist_write, "hist_read": hist_read}


norm_eps = 1e-05

def conv_update(history, current, conv_taps, live_mask):
    kept_hist = history.astype(jnp.float32) * live_mask[:, :, None]
    mixed_sum = lax.optimization_barrier(jnp.sum(kept_hist * conv_taps[None, :-1, :], axis=1)) + current.astype(jnp.float32) * conv_taps[-1][None, :]
    fresh_hist = jnp.concatenate([kept_hist[:, 1:].astype(jnp.bfloat16), current[:, None, :]], axis=1)
    return (jax.nn.silu(mixed_sum), fresh_hist)

def reference(tokens, lengths, norm_gain, w_gate, w_value, w_write, w_read, w_step, step_bias, decay_rate, skip_gain, conv_value_w, conv_write_w, conv_read_w, group_gain, w_out, state, hist_value, hist_write, hist_read):
    seq_total = tokens.shape[0]
    hist_len = KERNEL - 1
    offsets = hist_len - jnp.arange(hist_len, dtype=jnp.int32)
    live_mask = (offsets[None, :] <= lengths[:, None]).astype(jnp.float32)
    per_group = HEADS // GROUPS
    current = tokens
    states_out, values_out, writes_out, reads_out = ([], [], [], [])
    for layer_idx in range(2):
        floats = current.astype(jnp.float32)
        row_scale = lax.rsqrt(lax.optimization_barrier(jnp.mean(floats * floats, axis=1)) + norm_eps)
        normed = (floats * row_scale[:, None] * norm_gain[layer_idx][None, :]).astype(jnp.bfloat16)
        gate_part = jnp.dot(normed, w_gate[layer_idx], preferred_element_type=jnp.float32).astype(jnp.bfloat16)
        value_part = jnp.dot(normed, w_value[layer_idx], preferred_element_type=jnp.float32).astype(jnp.bfloat16)
        write_part = jnp.dot(normed, w_write[layer_idx], preferred_element_type=jnp.float32).astype(jnp.bfloat16)
        read_part = jnp.dot(normed, w_read[layer_idx], preferred_element_type=jnp.float32).astype(jnp.bfloat16)
        step_raw = jnp.dot(normed, w_step[layer_idx], preferred_element_type=jnp.float32)
        value_act, value_hist = conv_update(hist_value[layer_idx], value_part, conv_value_w[layer_idx], live_mask)
        write_act, write_hist = conv_update(hist_write[layer_idx], write_part, conv_write_w[layer_idx], live_mask)
        read_act, read_hist = conv_update(hist_read[layer_idx], read_part, conv_read_w[layer_idx], live_mask)
        step_size = jax.nn.softplus(step_raw + step_bias[layer_idx][None, :])
        decay_keep = jnp.exp(-decay_rate[layer_idx][None, :] * step_size)
        write_groups = jnp.swapaxes(write_act.reshape(seq_total, STATE, GROUPS), 1, 2)
        read_groups = jnp.swapaxes(read_act.reshape(seq_total, STATE, GROUPS), 1, 2)
        write_heads = jnp.repeat(write_groups, per_group, axis=1)
        read_heads = jnp.repeat(read_groups, per_group, axis=1)
        inputs = value_act.reshape(seq_total, HEADS, HEAD_DIM)
        updated = decay_keep[:, :, None, None] * state[layer_idx] + (step_size[:, :, None] * inputs)[:, :, :, None] * write_heads[:, :, None, :]
        readout = jnp.einsum('shpn,shn->shp', updated, read_heads, precision=lax.Precision.HIGHEST) + skip_gain[layer_idx][None, :, None] * inputs
        gated_out = readout.reshape(seq_total, WIDTH) * jax.nn.silu(gate_part.astype(jnp.float32))
        grouped = gated_out.reshape(seq_total, GROUPS, WIDTH // GROUPS)
        grouped = grouped * lax.rsqrt(lax.optimization_barrier(jnp.mean(grouped * grouped, axis=2, keepdims=True)) + norm_eps)
        mixer_out = (grouped.reshape(seq_total, WIDTH) * group_gain[layer_idx][None, :]).astype(jnp.bfloat16)
        current = jnp.dot(mixer_out, w_out[layer_idx], preferred_element_type=jnp.float32)
        if layer_idx == 0:
            current = current.astype(jnp.bfloat16)
        states_out.append(updated)
        values_out.append(value_hist)
        writes_out.append(write_hist)
        reads_out.append(read_hist)
    return (current, jnp.stack(states_out), jnp.stack(values_out), jnp.stack(writes_out), jnp.stack(reads_out))
```

```python
import functools

import jax
import jax.numpy as jnp
from jax import lax
from jax.experimental import pallas as pl
from jax.experimental.pallas import tpu as pltpu
from jax.sharding import PartitionSpec as P

MESH = pl.DeviceIdType.MESH
F32 = jnp.float32
BF16 = jnp.bfloat16
EPS = 1e-05

T0, IN0, IN1, OUT0, OUT1, GAIN, WR0, RS0, AG0, WR1, RS1 = range(11)


def iota(shape, dim):
    return lax.broadcasted_iota(jnp.int32, shape, dim)


def silu(x):
    return x / (1.0 + jnp.exp(-x))


def as_column(row):
    n = row.shape[1]
    square = jnp.broadcast_to(row, (n, n))
    return jnp.sum(jnp.where(iota((n, n), 0) == iota((n, n), 1), square, 0.0), axis=1, keepdims=True)


def dot(a, b, ca, cb):
    return lax.dot_general(a, b, (((ca,), (cb,)), ((), ())), preferred_element_type=F32)


def kernel(
    tok, lengths, ngain, wg, wv, ww, wr, ws, sb, dr, sg, cv, cw, cr, gg, wo, state, hv, hw, hr,
    mixed, nstate, nhv, nhw, nhr,
    tile_x, xbuf, wst, wfull, wofull, gain, st, nst, sel_n, cbv, t3v, cbwr, t3wr, ggc, wrsend, wrbuf, keepb, rsend, rbuf,
    ssem, rsem, lsem,
):
    t = lax.axis_index("tp")
    d = lax.axis_index("dp")
    z, y = t >> 2, t & 3
    own = z == d

    def dev(td, dd):
        return {"tp": td, "dp": dd}

    def send(src, dst, ex, td, dd):
        pltpu.make_async_remote_copy(
            src_ref=src, dst_ref=dst, send_sem=ssem.at[ex], recv_sem=rsem.at[ex],
            device_id=dev(td, dd), device_id_type=MESH,
        ).start()

    def wait(ref, sem):
        pltpu.make_async_copy(ref, ref, sem).wait()

    def wait_31_or_32(ref, sem):
        @pl.when(own)
        def _():
            wait(ref.at[0:31], sem)

        @pl.when(jnp.logical_not(own))
        def _():
            wait(ref, sem)

    def far_first(i):
        q, p = i >> 2, i & 3
        dz = 4 + (1 - 2 * (q & 1)) * ((q + 1) >> 1)
        dy = 2 + (1 - 2 * (p & 1)) * ((p + 1) >> 1)
        return (((z + dz) & 7) << 2) + ((y + dy) & 3)

    bar = pltpu.get_barrier_semaphore()

    def greet_tp(i, c):
        pl.semaphore_signal(bar, inc=1, device_id=dev(far_first(i), d), device_id_type=MESH)
        return c

    def greet_dp(i, c):
        pl.semaphore_signal(bar, inc=1, device_id=dev(t, (d + i) & 7), device_id_type=MESH)
        return c

    def greet_across(i, c):
        dd, td = i >> 2, 4 * d + (i & 3)

        @pl.when(jnp.logical_not((dd == d) & (td == t)))
        def _():
            pl.semaphore_signal(bar, inc=1, device_id=dev(td, dd), device_id_type=MESH)

        return c

    lax.fori_loop(0, 32, greet_across, 0)
    lax.fori_loop(0, 31, greet_tp, 0)
    lax.fori_loop(1, 8, greet_dp, 0)

    load = [pltpu.make_async_copy(state.at[l], st.at[l], lsem.at[l]) for l in range(2)]
    for l in range(2):
        load[l].start()

    tile_x[...] = jnp.zeros((8, 128), BF16)
    tile_x[0:6, :] = tok[...]
    for l in range(2):
        wst[l, 0:64, :] = wv[l]
        wst[l, 64:128, :] = wg[l]
        tail = jnp.concatenate(
            [ww[l].astype(F32), wr[l].astype(F32), ws[0, l : l + 1, :].astype(F32), jnp.zeros((15, 128), F32)], axis=0
        )
        wst[l, 128:160, :] = tail.astype(BF16)
        wfull[l, :, pl.ds(pl.multiple_of(d * 128, 128), 128)] = wst[l]
        wofull[l, :, pl.ds(pl.multiple_of(d * 128, 128), 128)] = wo[l]
    gain[:, pl.ds(pl.multiple_of(d * 128, 128), 128)] = ngain[...]

    srow = iota((24, 32), 0)
    six = (srow >= 6).astype(jnp.int32) + (srow >= 12).astype(jnp.int32) + (srow >= 18).astype(jnp.int32)
    place = (srow + 2 * six == iota((24, 32), 1)).astype(F32)
    place_b = place.astype(BF16)
    len_row = lengths[...].astype(F32)
    len_pad = jnp.dot(jnp.broadcast_to(len_row, (8, 24)).astype(BF16), place_b, preferred_element_type=F32)[0:1]
    len_col = as_column(len_row)
    for l in range(2):
        base_v = jnp.zeros((64, 32), F32)
        base_wr = jnp.zeros((16, 32), F32)
        for k in range(3):
            live_pad = (len_pad >= float(3 - k)).astype(F32)
            base_v += as_column(cv[l, k : k + 1, :]) * (dot(hv[l, k], place_b, 0, 0) * live_pad)
            base_w = as_column(cw[l, k : k + 1, :]) * (dot(hw[l, k], place_b, 1, 0) * live_pad)
            base_r = as_column(cr[l, k : k + 1, :]) * (dot(hr[l, k], place_b, 1, 0) * live_pad)
            base_wr += jnp.concatenate([base_w, base_r], axis=0)
            if k > 0:
                live_row = (len_row >= float(3 - k)).astype(F32)
                live_col = (len_col >= float(3 - k)).astype(F32)
                nhv[l, k - 1] = (hv[l, k].astype(F32) * live_col).astype(BF16)
                nhw[l, k - 1] = (hw[l, k].astype(F32) * live_row).astype(BF16)
                nhr[l, k - 1] = (hr[l, k].astype(F32) * live_row).astype(BF16)
        cbv[l] = base_v
        cbwr[l] = base_wr
        t3v[l] = jnp.broadcast_to(as_column(cv[l, 3:4, :]), (64, 32))
        t3wr[l] = jnp.broadcast_to(
            jnp.concatenate([as_column(cw[l, 3:4, :]), as_column(cr[l, 3:4, :])], axis=0), (16, 32)
        )
        ggc[l] = jnp.broadcast_to(as_column(gg[l : l + 1, :]), (64, 32))
    group = (t >= 16).astype(jnp.int32)
    sel_row = iota((256, 128), 0)
    sel_n[...] = (((sel_row >> 1) == iota((256, 128), 1)) & ((sel_row & 1) == group)).astype(F32).astype(BF16)

    pl.semaphore_wait(bar, 70 - own.astype(jnp.int32))

    def tokens_out(i, c):
        td = far_first(i)

        @pl.when(jnp.logical_not(own & (td == t)))
        def _():
            send(tile_x, xbuf.at[0, 4 * d + y], T0, td, z)

        return c

    lax.fori_loop(0, 32, tokens_out, 0)

    @pl.when(own)
    def _():
        xbuf[0, 4 * d + y] = tile_x[...]

    def weights_out(i, c):
        dd = (d + i) & 7
        col = pl.ds(pl.multiple_of(d * 128, 128), 128)
        send(ngain, gain.at[:, col], GAIN, t, dd)
        send(wst.at[0], wfull.at[0, :, col], IN0, t, dd)
        return c

    def weights_later(i, c):
        dd = (d + i) & 7
        col = pl.ds(pl.multiple_of(d * 128, 128), 128)
        send(wo.at[0], wofull.at[0, :, col], OUT0, t, dd)
        send(wst.at[1], wfull.at[1, :, col], IN1, t, dd)
        send(wo.at[1], wofull.at[1, :, col], OUT1, t, dd)
        return c

    lax.fori_loop(1, 8, weights_out, 0)
    lax.fori_loop(1, 8, weights_later, 0)

    wait_31_or_32(xbuf.at[0], rsem.at[T0])

    wait(gain.at[:, 0:896], rsem.at[GAIN])

    lane = iota((64, 32), 1)
    sub8 = iota((8, 128), 0)
    lane8 = iota((8, 128), 1)
    store = []
    for l in range(2):
        xs = [xbuf[l, 4 * a : 4 * a + 4].astype(F32).reshape(32, 128) for a in range(8)]
        squares = xs[0] * xs[0]
        for a in range(1, 8):
            squares += xs[a] * xs[a]
        scale = lax.rsqrt(jnp.sum(squares, axis=1, keepdims=True) / 1024.0 + EPS)
        normed = jnp.concatenate(
            [(xs[a] * scale * gain[l : l + 1, 128 * a : 128 * a + 128]).astype(BF16) for a in range(8)], axis=1
        )
        wait(wfull.at[l, :, 0:896], rsem.at[IN0 if l == 0 else IN1])
        proj = dot(wfull[l], normed, 1, 1)
        wr_new = proj[128:144].astype(BF16)
        wr_act = silu(cbwr[l] + t3wr[l] * wr_new.astype(F32))
        wr_tile = jnp.concatenate([wr_act[0:8], wr_act[8:16], jnp.zeros((8, 64), F32)], axis=1).astype(BF16)
        wrsend[l] = wr_tile
        ex = WR0 if l == 0 else WR1

        def maps_out(i, c):
            send(wrsend.at[l], wrbuf.at[l, t], ex, far_first(i), d)
            return c

        lax.fori_loop(0, 31, maps_out, 0)
        wrbuf[l, t] = wr_tile

        value_new = proj[0:64].astype(BF16)
        u = silu(cbv[l] + t3v[l] * value_new.astype(F32))
        gate = silu(proj[64:128].astype(BF16).astype(F32))
        raw = proj[144:145] + sb[0:1, l : l + 1]
        step = jnp.maximum(raw, 0.0) + jnp.log1p(jnp.exp(-jnp.abs(raw)))
        keep = jnp.exp(-dr[0:1, l : l + 1] * step)
        keepb[...] = jnp.broadcast_to(as_column(keep), (32, 128))
        su = u * step
        nhv[l, 2] = dot(place_b, value_new, 1, 1).astype(BF16)
        wr_nat = dot(wr_new, place_b, 1, 1)
        nhw[l, 2] = wr_nat[0:8].astype(BF16)
        nhr[l, 2] = wr_nat[8:16].astype(BF16)
        load[l].wait()

        wait(wrbuf.at[l, 0:31], rsem.at[ex])
        maps = dot(wrbuf[l].reshape(256, 128), sel_n[...], 0, 0)
        w_map = maps[0:32].astype(BF16)
        r_map = maps[32:64].astype(BF16)

        readout = jnp.zeros((64, 32), F32)
        for s in range(24):
            p = s + 2 * (s // 6)
            outer = dot(jnp.where(lane == p, su, 0.0).astype(BF16), w_map, 1, 0)
            new = keepb[p : p + 1, :] * st[l, s] + outer
            nst[l, s] = new
            readout = jnp.where(lane == p, dot(new.astype(BF16), r_map, 1, 1), readout)
        out_copy = pltpu.make_async_copy(nst.at[l], nstate.at[l], lsem.at[2 + l])
        out_copy.start()
        store.append(out_copy)

        gated = (readout + sg[0:1, l : l + 1] * u) * gate
        sq = jnp.sum(gated * gated, axis=0, keepdims=True)
        sq_hi = sq.astype(BF16).astype(F32)
        sq_lo = sq - sq_hi
        pad = jnp.zeros((1, 96), F32)
        row_hi = jnp.concatenate([sq_hi, pad], axis=1)
        row_lo = jnp.concatenate([sq_lo, pad], axis=1)
        mixer = (gated * ggc[l]).astype(BF16)
        wait(wofull.at[l, :, 0:896], rsem.at[OUT0 if l == 0 else OUT1])
        part = dot(mixer, wofull[l], 0, 0)
        for a in range(8):
            for k in range(4):
                piece = part[8 * k : 8 * k + 8, 128 * a : 128 * a + 128]
                piece = jnp.where(sub8 == 6, row_hi, jnp.where(sub8 == 7, row_lo, piece))
                rsend[l, 4 * a + k] = piece.astype(BF16)

        if l == 0:

            def parts_out(i, c):
                td = far_first(i)
                send(rsend.at[0, td], rbuf.at[0, t], RS0, td, d)
                return c

            lax.fori_loop(0, 31, parts_out, 0)
            rbuf[0, t] = rsend[0, t]
            wait(rbuf.at[0, 0:31], rsem.at[RS0])
        else:

            def parts_across(i, c):
                dd, td = i >> 2, 4 * d + (i & 3)

                @pl.when(jnp.logical_not((dd == d) & (td == t)))
                def _():
                    send(rsend.at[1, i], rbuf.at[1, t], RS1, td, dd)

                return c

            lax.fori_loop(0, 32, parts_across, 0)

            @pl.when(own)
            def _():
                rbuf[1, t] = rsend[1, t]

            wait_31_or_32(rbuf.at[1], rsem.at[RS1])

        total = jnp.zeros((8, 128), F32)
        for g in range(2):
            acc = jnp.sum(rbuf[l, 16 * g : 16 * g + 16].astype(F32), axis=0)
            sq_row = acc[6:7] + acc[7:8]
            sq_col = jnp.sum(
                jnp.where(lane8 == sub8 + 8 * y, jnp.broadcast_to(sq_row, (8, 128)), 0.0), axis=1, keepdims=True
            )
            total += acc * lax.rsqrt(sq_col / 1024.0 + EPS)
        if l == 0:
            tile = jnp.where(sub8 < 6, total, 0.0).astype(BF16)
            rsend[0, t] = tile

            def hidden_out(i, c):
                send(rsend.at[0, t], xbuf.at[1, t], AG0, far_first(i), d)
                return c

            lax.fori_loop(0, 31, hidden_out, 0)
            xbuf[1, t] = tile
            wait(xbuf.at[1, 0:31], rsem.at[AG0])
        else:
            mixed[...] = total[0:6]

    wait_31_or_32(xbuf.at[0], ssem.at[T0])
    wait_31_or_32(rbuf.at[1], ssem.at[RS1])
    wait(gain.at[:, 0:896], ssem.at[GAIN])
    for l in range(2):
        wait(wfull.at[l, :, 0:896], ssem.at[IN0 if l == 0 else IN1])
        wait(wofull.at[l, :, 0:896], ssem.at[OUT0 if l == 0 else OUT1])
        wait(wrbuf.at[l, 0:31], ssem.at[WR0 if l == 0 else WR1])
    wait(rbuf.at[0, 0:31], ssem.at[RS0])
    wait(xbuf.at[1, 0:31], ssem.at[AG0])
    for out_copy in store:
        out_copy.wait()


def local(
    tokens, lengths, norm_gain, w_gate, w_value, w_write, w_read, w_step, step_bias, decay_rate, skip_gain,
    conv_value_w, conv_write_w, conv_read_w, group_gain, w_out, state, hist_value, hist_write, hist_read,
):
    def flip(w):
        return jnp.transpose(w, (0, 2, 1))

    args = (
        tokens, lengths.reshape(1, 24), norm_gain, flip(w_gate), flip(w_value), flip(w_write), flip(w_read),
        jnp.transpose(w_step, (2, 0, 1)), step_bias.T, decay_rate.T, skip_gain.T,
        conv_value_w, conv_write_w, conv_read_w, group_gain, w_out, state.reshape(2, 24, 64, 128),
        jnp.transpose(hist_value, (0, 2, 1, 3)), jnp.transpose(hist_write, (0, 2, 3, 1)),
        jnp.transpose(hist_read, (0, 2, 3, 1)),
    )
    vmem = pl.BlockSpec(memory_space=pltpu.VMEM)
    hbm = pl.BlockSpec(memory_space=pl.ANY)
    mixed, nstate, nhv, nhw, nhr = pl.pallas_call(
        kernel,
        out_shape=(
            jax.ShapeDtypeStruct((6, 128), F32),
            jax.ShapeDtypeStruct((2, 24, 64, 128), F32),
            jax.ShapeDtypeStruct((2, 3, 24, 64), BF16),
            jax.ShapeDtypeStruct((2, 3, 8, 24), BF16),
            jax.ShapeDtypeStruct((2, 3, 8, 24), BF16),
        ),
        in_specs=[vmem] * 16 + [hbm] + [vmem] * 3,
        out_specs=(vmem, hbm, vmem, vmem, vmem),
        scratch_shapes=[
            pltpu.VMEM((8, 128), BF16),
            pltpu.VMEM((2, 32, 8, 128), BF16),
            pltpu.VMEM((2, 160, 128), BF16),
            pltpu.VMEM((2, 160, 1024), BF16),
            pltpu.VMEM((2, 64, 1024), BF16),
            pltpu.VMEM((2, 1024), F32),
            pltpu.VMEM((2, 24, 64, 128), F32),
            pltpu.VMEM((2, 24, 64, 128), F32),
            pltpu.VMEM((256, 128), BF16),
            pltpu.VMEM((2, 64, 32), F32),
            pltpu.VMEM((2, 64, 32), F32),
            pltpu.VMEM((2, 16, 32), F32),
            pltpu.VMEM((2, 16, 32), F32),
            pltpu.VMEM((2, 64, 32), F32),
            pltpu.VMEM((2, 8, 128), BF16),
            pltpu.VMEM((2, 32, 8, 128), BF16),
            pltpu.VMEM((32, 128), F32),
            pltpu.VMEM((2, 32, 8, 128), BF16),
            pltpu.VMEM((2, 32, 8, 128), BF16),
                pltpu.SemaphoreType.DMA((11,)),
            pltpu.SemaphoreType.DMA((11,)),
            pltpu.SemaphoreType.DMA((4,)),
        ],
        compiler_params=pltpu.CompilerParams(collective_id=0, has_side_effects=True),
    )(*args)
    return (
        mixed,
        nstate.reshape(2, 24, 1, 64, 128),
        jnp.transpose(nhv, (0, 2, 1, 3)),
        jnp.transpose(nhw, (0, 3, 1, 2)),
        jnp.transpose(nhr, (0, 3, 1, 2)),
    )


def solution(mesh):
    return jax.shard_map(
        local,
        mesh=mesh,
        in_specs=(
            P("tp", "dp"),
            P("dp"),
            P(None, "dp"),
            P(None, "dp", "tp"),
            P(None, "dp", "tp"),
            P(None, "dp", "tp"),
            P(None, "dp", "tp"),
            P(None, "dp", "tp"),
            P(None, "tp"),
            P(None, "tp"),
            P(None, "tp"),
            P(None, None, "tp"),
            P(None, None, "tp"),
            P(None, None, "tp"),
            P(None, "tp"),
            P(None, "tp", "dp"),
            P(None, "dp", "tp", None, None),
            P(None, "dp", None, "tp"),
            P(None, "dp", None, "tp"),
            P(None, "dp", None, "tp"),
        ),
        out_specs=(
            P("tp", "dp"),
            P(None, "dp", "tp", None, None),
            P(None, "dp", None, "tp"),
            P(None, "dp", None, "tp"),
            P(None, "dp", None, "tp"),
        ),
        check_vma=False,
    )
```

```python
import functools

import jax
import jax.numpy as jnp
from jax import lax
from jax.experimental import pallas as pl
from jax.experimental.pallas import tpu as pltpu
from jax.sharding import PartitionSpec as P

MESH = pl.DeviceIdType.MESH
F32 = jnp.float32
BF16 = jnp.bfloat16
EPS = 1e-05

T0, GAIN, INW0, INW1, IN0, IN1, OUT0, OUT1, WR0, CB, WP, RS0, AG0, RS1 = range(14)
EXCHANGES = 14


def iota(shape, dim):
    return lax.broadcasted_iota(jnp.int32, shape, dim)


def silu(x):
    return x / (1.0 + jnp.exp(-x))


def as_column(row):
    n = row.shape[1]
    square = jnp.broadcast_to(row, (n, n))
    return jnp.sum(jnp.where(iota((n, n), 0) == iota((n, n), 1), square, 0.0), axis=1, keepdims=True)


def as_row(column):
    n = column.shape[0]
    square = jnp.broadcast_to(column, (n, n))
    return jnp.sum(jnp.where(iota((n, n), 0) == iota((n, n), 1), square, 0.0), axis=0, keepdims=True)


def dot(a, b, ca, cb):
    return lax.dot_general(a, b, (((ca,), (cb,)), ((), ())), preferred_element_type=F32)


def kernel(
    tok, lengths, ngain, wg, wv, ww, wr, ws, sb, dr, sg, cv, cw, cr, gg, wo, state, hv, hw, hr,
    mixed, nstate, nhv, nhw, nhr,
    tile_x, xbuf, wst, wfull, wofull, gain, st, stb, sel, cbv, t3v, cbwr, t3wr, ggc,
    wrsend, wrbuf, rsend, rbuf, agsend, agbuf, cbsend, cbbuf, wpsend, wpbuf, wperm, keepb,
    ssem, rsem, lsem,
):
    t = lax.axis_index("tp")
    d = lax.axis_index("dp")
    z, y = t >> 2, t & 3
    own = z == d
    col = pl.ds(pl.multiple_of(d * 128, 128), 128)

    def dev(td, dd):
        return {"tp": td, "dp": dd}

    def send(src, dst, ex, td, dd):
        pltpu.make_async_remote_copy(
            src_ref=src, dst_ref=dst, send_sem=ssem.at[ex], recv_sem=rsem.at[ex],
            device_id=dev(td, dd), device_id_type=MESH,
        ).start()

    def wait(ref, sem):
        pltpu.make_async_copy(ref, ref, sem).wait()

    def wait_31_or_32(part, ref, sem):
        @pl.when(own)
        def _():
            wait(part, sem)

        @pl.when(jnp.logical_not(own))
        def _():
            wait(ref, sem)

    def far_first(i):
        q, p = i >> 2, i & 3
        dz = 4 + (1 - 2 * (q & 1)) * ((q + 1) >> 1)
        dy = 2 + (1 - 2 * (p & 1)) * ((p + 1) >> 1)
        return (((z + dz) & 7) << 2) + ((y + dy) & 3)

    def to_tp(body):
        def step(i, c):
            body(far_first(i))
            return c

        lax.fori_loop(0, 31, step, 0)

    def to_dp(body):
        def step(i, c):
            body((d + i) & 7)
            return c

        lax.fori_loop(1, 8, step, 0)

    def to_across(body):
        def step(i, c):
            dd, td = i >> 2, 4 * d + (i & 3)

            @pl.when(jnp.logical_not((dd == d) & (td == t)))
            def _():
                body(i, td, dd)

            return c

        lax.fori_loop(0, 32, step, 0)

    bar = pltpu.get_barrier_semaphore()

    def greet(td, dd):
        pl.semaphore_signal(bar, inc=1, device_id=dev(td, dd), device_id_type=MESH)

    to_across(lambda i, td, dd: greet(td, dd))
    to_tp(lambda td: greet(td, d))
    to_dp(lambda dd: greet(t, dd))

    load = [pltpu.make_async_copy(state.at[l], st.at[l], lsem.at[l]) for l in range(2)]
    for l in range(2):
        load[l].start()
    tile_x[...] = jnp.zeros((8, 128), BF16)
    tile_x[0:6, :] = tok[...]
    for l in range(2):
        head = jnp.concatenate(
            [ww[l].astype(F32), wr[l].astype(F32), ws[0, l : l + 1, :].astype(F32), jnp.zeros((15, 128), F32)], axis=0
        )
        wst[l, 0:32, :] = head.astype(BF16)
        wst[l, 32:96, :] = wv[l]
        wst[l, 96:160, :] = wg[l]

    pl.semaphore_wait(bar, 70 - own.astype(jnp.int32))

    def tokens_out(i, c):
        td = far_first(i)

        @pl.when(jnp.logical_not(own & (td == t)))
        def _():
            send(tile_x, xbuf.at[4 * d + y], T0, td, z)

        return c

    lax.fori_loop(0, 32, tokens_out, 0)

    @pl.when(own)
    def _():
        xbuf[4 * d + y] = tile_x[...]

    def first_weights(dd):
        send(ngain, gain.at[:, col], GAIN, t, dd)
        send(wst.at[0, 0:32], wfull.at[0, 0:32, col], INW0, t, dd)
        send(wst.at[1, 0:32], wfull.at[1, 0:32, col], INW1, t, dd)

    to_dp(first_weights)
    to_dp(lambda dd: send(wst.at[0, 32:160], wfull.at[0, 32:160, col], IN0, t, dd))
    to_dp(lambda dd: send(wo.at[0], wofull.at[0, :, col], OUT0, t, dd))
    to_dp(lambda dd: send(wst.at[1, 32:160], wfull.at[1, 32:160, col], IN1, t, dd))
    to_dp(lambda dd: send(wo.at[1], wofull.at[1, :, col], OUT1, t, dd))

    for l in range(2):
        wfull[l, :, col] = wst[l]
        wofull[l, :, col] = wo[l]
    gain[:, col] = ngain[...]
    srow = iota((24, 32), 0)
    six = (srow >= 6).astype(jnp.int32) + (srow >= 12).astype(jnp.int32) + (srow >= 18).astype(jnp.int32)
    place_b = (srow + 2 * six == iota((24, 32), 1)).astype(F32).astype(BF16)
    len_row = lengths[...].astype(F32)
    len_pad = jnp.dot(jnp.broadcast_to(len_row, (8, 24)).astype(BF16), place_b, preferred_element_type=F32)[0:1]
    len_col = as_column(len_row)
    for l in range(2):
        base_v = jnp.zeros((64, 32), F32)
        base_wr = jnp.zeros((16, 32), F32)
        for k in range(3):
            live_pad = (len_pad >= float(3 - k)).astype(F32)
            base_v += as_column(cv[l, k : k + 1, :]) * (dot(hv[l, k], place_b, 0, 0) * live_pad)
            base_w = as_column(cw[l, k : k + 1, :]) * (dot(hw[l, k], place_b, 1, 0) * live_pad)
            base_r = as_column(cr[l, k : k + 1, :]) * (dot(hr[l, k], place_b, 1, 0) * live_pad)
            base_wr += jnp.concatenate([base_w, base_r], axis=0)
            if k > 0:
                live_row = (len_row >= float(3 - k)).astype(F32)
                live_col = (len_col >= float(3 - k)).astype(F32)
                nhv[l, k - 1] = (hv[l, k].astype(F32) * live_col).astype(BF16)
                nhw[l, k - 1] = (hw[l, k].astype(F32) * live_row).astype(BF16)
                nhr[l, k - 1] = (hr[l, k].astype(F32) * live_row).astype(BF16)
        cbv[l] = base_v
        t3v[l] = jnp.broadcast_to(as_column(cv[l, 3:4, :]), (64, 32))
        tap_w = jnp.broadcast_to(as_column(cw[l, 3:4, :]), (8, 32))
        tap_r = jnp.broadcast_to(as_column(cr[l, 3:4, :]), (8, 32))
        if l == 0:
            cbwr[...] = base_wr
            t3wr[...] = jnp.concatenate([tap_w, tap_r], axis=0)
        else:
            cbsend[...] = jnp.concatenate([base_wr[0:8], base_wr[8:16], tap_w, tap_r], axis=1)
        ggc[l] = jnp.broadcast_to(as_column(gg[l : l + 1, :]), (64, 32))
    group = (t >= 16).astype(jnp.int32)
    sel_row = iota((256, 128), 0)
    for g in range(2):
        sel[g] = (((sel_row >> 1) == iota((256, 128), 1)) & ((sel_row & 1) == g)).astype(F32).astype(BF16)
    for l in range(2):
        load[l].wait()
        for s in range(24):
            stb[l, 64 * s : 64 * s + 64, :] = st[l, s].astype(BF16)

    wait_31_or_32(xbuf.at[0:31], xbuf, rsem.at[T0])
    wait(gain.at[:, 0:896], rsem.at[GAIN])

    lane = iota((64, 32), 1)
    sub8 = iota((8, 128), 0)
    lane8 = iota((8, 128), 1)
    for l in range(2):
        source = [xbuf[4 * a : 4 * a + 4] if l == 0 else agbuf[4 * a : 4 * a + 4, 0] for a in range(8)]
        xs = [x.astype(F32).reshape(32, 128) for x in source]
        squares = xs[0] * xs[0]
        for a in range(1, 8):
            squares += xs[a] * xs[a]
        scale = lax.rsqrt(jnp.sum(squares, axis=1, keepdims=True) / 1024.0 + EPS)
        normed = jnp.concatenate(
            [(xs[a] * scale * gain[l : l + 1, 128 * a : 128 * a + 128]).astype(BF16) for a in range(8)], axis=1
        )
        if l == 0:
            wait(wfull.at[0, 0:32, 0:896], rsem.at[INW0])
            first = dot(wfull[0, 0:32, :], normed, 1, 1)
            wr_new = first[0:16].astype(BF16)
            wr_act = silu(cbwr[...] + t3wr[...] * wr_new.astype(F32))
            wr_tile = jnp.concatenate([wr_act[0:8], wr_act[8:16], jnp.zeros((8, 64), F32)], axis=1).astype(BF16)
            wrsend[...] = wr_tile
            to_tp(lambda td: send(wrsend, wrbuf.at[t], WR0, td, d))
            wrbuf[t] = wr_tile
            wait(wfull.at[1, 0:32, 0:896], rsem.at[INW1])
            map_rows = wfull[1, 0:16, :].astype(F32)
            wpsend[0] = map_rows[0:8].astype(BF16)
            wpsend[1] = map_rows[8:16].astype(BF16)

            def piece_rows(td):
                return wpsend.at[:, :, pl.ds(pl.multiple_of((td >> 2) * 128, 128), 128)]

            to_tp(lambda td: send(piece_rows(td), wpbuf.at[:, t], WP, td, d))
            for m in range(2):
                wpbuf[m, t] = wpsend[m, :, pl.ds(pl.multiple_of(z * 128, 128), 128)]
            wait(wfull.at[0, 32:160, 0:896], rsem.at[IN0])
            rest = dot(wfull[0, 32:160, :], normed, 1, 1)
        else:
            wait(wfull.at[1, 32:160, 0:896], rsem.at[IN1])
            first = dot(wfull[1], normed, 1, 1)
            wr_new = first[0:16].astype(BF16)
            rest = first[32:160]
            maps = []
            for m in range(2):
                raw_map = agbuf[0:4, 1 + m].astype(F32)
                for a in range(1, 8):
                    raw_map += agbuf[4 * a : 4 * a + 4, 1 + m].astype(F32)
                new_map = (raw_map.reshape(32, 128) * scale).astype(BF16).astype(F32)
                maps.append(silu(conv_maps[32 * m : 32 * m + 32] + conv_maps[64 + 32 * m : 96 + 32 * m] * new_map))
            w_map, r_map = maps

        value_new = rest[0:64].astype(BF16)
        u = silu(cbv[l] + t3v[l] * value_new.astype(F32))
        gate = silu(rest[64:128].astype(BF16).astype(F32))
        raw = first[16:17] + sb[0:1, l : l + 1]
        step = jnp.maximum(raw, 0.0) + jnp.log1p(jnp.exp(-jnp.abs(raw)))
        keep = jnp.exp(-dr[0:1, l : l + 1] * step)
        su = u * step
        if l == 0:
            wait(wrbuf.at[0:31], rsem.at[WR0])
            maps = dot(wrbuf[...].reshape(256, 128), sel[group], 0, 0)
            w_map, r_map = maps[0:32], maps[32:64]
        r_b = r_map.astype(BF16)
        stored = dot(stb[l], r_b, 1, 1)
        readout = jnp.zeros((64, 32), F32)
        for s in range(24):
            p = s + 2 * (s // 6)
            readout = jnp.where(lane == p, stored[64 * s : 64 * s + 64], readout)
        wr_dot = as_row(jnp.sum(w_map * r_map, axis=1, keepdims=True))
        gated = (keep * readout + su * wr_dot + sg[0:1, l : l + 1] * u) * gate
        sq = jnp.sum(gated * gated, axis=0, keepdims=True)
        sq_hi = sq.astype(BF16).astype(F32)
        sq_lo = sq - sq_hi
        pad = jnp.zeros((1, 96), F32)
        row_hi = jnp.concatenate([sq_hi, pad], axis=1)
        row_lo = jnp.concatenate([sq_lo, pad], axis=1)
        mixer = (gated * ggc[l]).astype(BF16)
        wait(wofull.at[l, :, 0:896], rsem.at[OUT0 if l == 0 else OUT1])
        part = dot(mixer, wofull[l], 0, 0)
        for a in range(8):
            for k in range(4):
                piece = part[8 * k : 8 * k + 8, 128 * a : 128 * a + 128]
                piece = jnp.where(sub8 == 6, row_hi, jnp.where(sub8 == 7, row_lo, piece))
                rsend[l, 4 * a + k] = piece.astype(BF16)
        if l == 0:
            to_tp(lambda td: send(rsend.at[0, td], rbuf.at[0, t], RS0, td, d))
            rbuf[0, t] = rsend[0, t]
            to_tp(lambda td: send(cbsend, cbbuf.at[t], CB, td, d))
            cbbuf[t] = cbsend[...]
        else:
            to_across(lambda i, td, dd: send(rsend.at[1, i], rbuf.at[1, t], RS1, td, dd))

            @pl.when(own)
            def _():
                rbuf[1, t] = rsend[1, t]

        w_b = w_map.astype(BF16)
        keepb[...] = jnp.broadcast_to(as_column(keep), (32, 128))
        for s in range(24):
            p = s + 2 * (s // 6)
            outer = dot(jnp.where(lane == p, su, 0.0).astype(BF16), w_b, 1, 0)
            nstate[l, s] = keepb[p : p + 1, :] * st[l, s] + outer
        nhv[l, 2] = dot(place_b, value_new, 1, 1).astype(BF16)
        wr_nat = dot(wr_new, place_b, 1, 1)
        nhw[l, 2] = wr_nat[0:8].astype(BF16)
        nhr[l, 2] = wr_nat[8:16].astype(BF16)
        if l == 0:
            wait(wpbuf.at[:, 0:31], rsem.at[WP])
            for m in range(2):
                rows = wpbuf[m].reshape(256, 128)
                for g in range(2):
                    wperm[g, 128 * m : 128 * m + 128, :] = dot(sel[g], rows, 0, 0).astype(BF16)
            wait(rbuf.at[0, 0:31], rsem.at[RS0])
        else:
            wait_31_or_32(rbuf.at[1, 0:31], rbuf.at[1], rsem.at[RS1])

        total = jnp.zeros((8, 128), F32)
        for g in range(2):
            acc = jnp.sum(rbuf[l, 16 * g : 16 * g + 16].astype(F32), axis=0)
            sq_row = acc[6:7] + acc[7:8]
            sq_col = jnp.sum(
                jnp.where(lane8 == sub8 + 8 * y, jnp.broadcast_to(sq_row, (8, 128)), 0.0), axis=1, keepdims=True
            )
            total += acc * lax.rsqrt(sq_col / 1024.0 + EPS)
        if l == 0:
            tile = jnp.where(sub8 < 6, total, 0.0).astype(BF16)
            scaled = (tile.astype(F32) * gain[1:2, pl.ds(pl.multiple_of(z * 128, 128), 128)]).astype(BF16)
            for g in range(2):
                partial_maps = dot(scaled, wperm[g], 1, 1).astype(BF16)
                agsend[g, 0] = tile
                agsend[g, 1] = partial_maps[:, 0:128]
                agsend[g, 2] = partial_maps[:, 128:256]
            to_tp(lambda td: send(agsend.at[td >> 4], agbuf.at[t], AG0, td, d))
            agbuf[t] = agsend[group]
            wait(cbbuf.at[0:31], rsem.at[CB])
            conv_maps = lax.dot_general(
                cbbuf[...].reshape(256, 128), sel[group].astype(F32), (((0,), (0,)), ((), ())),
                precision=lax.Precision.HIGHEST, preferred_element_type=F32,
            )
            wait(agbuf.at[0:31], rsem.at[AG0])
        else:
            mixed[...] = total[0:6]

    wait_31_or_32(xbuf.at[0:31], xbuf, ssem.at[T0])
    wait_31_or_32(rbuf.at[1, 0:31], rbuf.at[1], ssem.at[RS1])
    wait(wpbuf.at[:, 0:31], ssem.at[WP])
    wait(gain.at[:, 0:896], ssem.at[GAIN])
    wait(wfull.at[0, 0:32, 0:896], ssem.at[INW0])
    wait(wfull.at[1, 0:32, 0:896], ssem.at[INW1])
    wait(wfull.at[0, 32:160, 0:896], ssem.at[IN0])
    wait(wfull.at[1, 32:160, 0:896], ssem.at[IN1])
    wait(wofull.at[0, :, 0:896], ssem.at[OUT0])
    wait(wofull.at[1, :, 0:896], ssem.at[OUT1])
    wait(wrbuf.at[0:31], ssem.at[WR0])
    wait(cbbuf.at[0:31], ssem.at[CB])
    wait(rbuf.at[0, 0:31], ssem.at[RS0])
    wait(agbuf.at[0:31], ssem.at[AG0])


def finish(*refs):
    given, outs, sem = refs[:5], refs[5:10], refs[10]
    copies = [pltpu.make_async_copy(a, b, sem.at[i]) for i, (a, b) in enumerate(zip(given, outs))]
    for copy in copies:
        copy.start()
    for copy in copies:
        copy.wait()


def local(
    tokens, lengths, norm_gain, w_gate, w_value, w_write, w_read, w_step, step_bias, decay_rate, skip_gain,
    conv_value_w, conv_write_w, conv_read_w, group_gain, w_out, state, hist_value, hist_write, hist_read,
):
    def flip(w):
        return jnp.transpose(w, (0, 2, 1))

    state = state.reshape(2, 24, 64, 128)
    args = (
        tokens, lengths.reshape(1, 24), norm_gain, flip(w_gate), flip(w_value), flip(w_write), flip(w_read),
        jnp.transpose(w_step, (2, 0, 1)), step_bias.T, decay_rate.T, skip_gain.T,
        conv_value_w, conv_write_w, conv_read_w, group_gain, w_out, state,
        jnp.transpose(hist_value, (0, 2, 1, 3)), jnp.transpose(hist_write, (0, 2, 3, 1)),
        jnp.transpose(hist_read, (0, 2, 3, 1)),
    )
    vmem = pl.BlockSpec(memory_space=pltpu.VMEM)
    hbm = pl.BlockSpec(memory_space=pl.ANY)
    outs = (
        ((6, 128), F32), ((2, 24, 64, 128), F32), ((2, 3, 24, 64), BF16), ((2, 3, 8, 24), BF16), ((2, 3, 8, 24), BF16),
    )
    held = pl.pallas_call(
        kernel,
        out_shape=tuple(pltpu.VMEM(*o) for o in outs),
        in_specs=[vmem] * 16 + [hbm] + [vmem] * 3,
        out_specs=(vmem,) * 5,
        scratch_shapes=[
            pltpu.VMEM((8, 128), BF16),
            pltpu.VMEM((32, 8, 128), BF16),
            pltpu.VMEM((2, 160, 128), BF16),
            pltpu.VMEM((2, 160, 1024), BF16),
            pltpu.VMEM((2, 64, 1024), BF16),
            pltpu.VMEM((2, 1024), F32),
            pltpu.VMEM((2, 24, 64, 128), F32),
            pltpu.VMEM((2, 1536, 128), BF16),
            pltpu.VMEM((2, 256, 128), BF16),
            pltpu.VMEM((2, 64, 32), F32),
            pltpu.VMEM((2, 64, 32), F32),
            pltpu.VMEM((16, 32), F32),
            pltpu.VMEM((16, 32), F32),
            pltpu.VMEM((2, 64, 32), F32),
            pltpu.VMEM((8, 128), BF16),
            pltpu.VMEM((32, 8, 128), BF16),
            pltpu.VMEM((2, 32, 8, 128), BF16),
            pltpu.VMEM((2, 32, 8, 128), BF16),
            pltpu.VMEM((2, 3, 8, 128), BF16),
            pltpu.VMEM((32, 3, 8, 128), BF16),
            pltpu.VMEM((8, 128), F32),
            pltpu.VMEM((32, 8, 128), F32),
            pltpu.VMEM((2, 8, 1024), BF16),
            pltpu.VMEM((2, 32, 8, 128), BF16),
            pltpu.VMEM((2, 256, 128), BF16),
            pltpu.VMEM((32, 128), F32),
            pltpu.SemaphoreType.DMA((EXCHANGES,)),
            pltpu.SemaphoreType.DMA((EXCHANGES,)),
            pltpu.SemaphoreType.DMA((2,)),
        ],
        compiler_params=pltpu.CompilerParams(collective_id=0, has_side_effects=True),
    )(*args)
    mixed, nstate, nhv, nhw, nhr = pl.pallas_call(
        finish,
        out_shape=tuple(jax.ShapeDtypeStruct(*o) for o in outs),
        in_specs=[vmem] * 5,
        out_specs=(hbm,) * 5,
        scratch_shapes=[pltpu.SemaphoreType.DMA((5,))],
    )(*(pltpu.with_memory_space_constraint(h, pltpu.VMEM) for h in held))
    return (
        mixed,
        nstate.reshape(2, 24, 1, 64, 128),
        jnp.transpose(nhv, (0, 2, 1, 3)),
        jnp.transpose(nhw, (0, 3, 1, 2)),
        jnp.transpose(nhr, (0, 3, 1, 2)),
    )


def solution(mesh):
    return jax.shard_map(
        local,
        mesh=mesh,
        in_specs=(
            P("tp", "dp"),
            P("dp"),
            P(None, "dp"),
            P(None, "dp", "tp"),
            P(None, "dp", "tp"),
            P(None, "dp", "tp"),
            P(None, "dp", "tp"),
            P(None, "dp", "tp"),
            P(None, "tp"),
            P(None, "tp"),
            P(None, "tp"),
            P(None, None, "tp"),
            P(None, None, "tp"),
            P(None, None, "tp"),
            P(None, "tp"),
            P(None, "tp", "dp"),
            P(None, "dp", "tp", None, None),
            P(None, "dp", None, "tp"),
            P(None, "dp", None, "tp"),
            P(None, "dp", None, "tp"),
        ),
        out_specs=(
            P("tp", "dp"),
            P(None, "dp", "tp", None, None),
            P(None, "dp", None, "tp"),
            P(None, "dp", None, "tp"),
            P(None, "dp", None, "tp"),
        ),
        check_vma=False,
    )
```

```python
import functools

import jax
import jax.numpy as jnp
from jax import lax
from jax.experimental import pallas as pl
from jax.experimental.pallas import tpu as pltpu
from jax.sharding import PartitionSpec as P

MESH = pl.DeviceIdType.MESH
F32 = jnp.float32
BF16 = jnp.bfloat16
EPS = 1e-05

T0, GAIN, INW0, INW1, IN0, IN1, OUT0, OUT1, WR0, CB, WP, RS0, AG0, RS1 = range(14)
EXCHANGES = 14


def iota(shape, dim):
    return lax.broadcasted_iota(jnp.int32, shape, dim)


def silu(x):
    return x / (1.0 + jnp.exp(-x))


def as_column(row):
    n = row.shape[1]
    square = jnp.broadcast_to(row, (n, n))
    return jnp.sum(jnp.where(iota((n, n), 0) == iota((n, n), 1), square, 0.0), axis=1, keepdims=True)


def as_row(column):
    n = column.shape[0]
    square = jnp.broadcast_to(column, (n, n))
    return jnp.sum(jnp.where(iota((n, n), 0) == iota((n, n), 1), square, 0.0), axis=0, keepdims=True)


def dot(a, b, ca, cb):
    return lax.dot_general(a, b, (((ca,), (cb,)), ((), ())), preferred_element_type=F32)


def kernel(*refs):
    given, state, outs, held, rest = refs[:19], refs[19], refs[20:25], refs[25:44], refs[44:]
    tok, lengths, ngain, wg, wv, ww, wr, ws, sb, dr, sg, cv, cw, cr, gg, wo, hv, hw, hr = held
    mixed, nstate, nhv, nhw, nhr = outs
    (
        tile_x, xbuf, wst, wfull, wofull, gain, st, stb, sel, cbv, t3v, cbwr, t3wr, ggc,
        wrsend, wrbuf, rsend, rbuf, agsend, agbuf, cbsend, cbbuf, wpsend, wpbuf, wperm, keepb,
        ssem, rsem, lsem, gsem,
    ) = rest
    t = lax.axis_index("tp")
    d = lax.axis_index("dp")
    z, y = t >> 2, t & 3
    own = z == d
    col = pl.ds(pl.multiple_of(d * 128, 128), 128)

    def dev(td, dd):
        return {"tp": td, "dp": dd}

    def send(src, dst, ex, td, dd):
        pltpu.make_async_remote_copy(
            src_ref=src, dst_ref=dst, send_sem=ssem.at[ex], recv_sem=rsem.at[ex],
            device_id=dev(td, dd), device_id_type=MESH,
        ).start()

    def wait(ref, sem):
        pltpu.make_async_copy(ref, ref, sem).wait()

    def wait_31_or_32(part, ref, sem):
        @pl.when(own)
        def _():
            wait(part, sem)

        @pl.when(jnp.logical_not(own))
        def _():
            wait(ref, sem)

    def far_first(i):
        q, p = i >> 2, i & 3
        dz = 4 + (1 - 2 * (q & 1)) * ((q + 1) >> 1)
        dy = 2 + (1 - 2 * (p & 1)) * ((p + 1) >> 1)
        return (((z + dz) & 7) << 2) + ((y + dy) & 3)

    def to_tp(body):
        def step(i, c):
            body(far_first(i))
            return c

        lax.fori_loop(0, 31, step, 0)

    def to_dp(body):
        def step(i, c):
            body((d + i) & 7)
            return c

        lax.fori_loop(1, 8, step, 0)

    def to_across(body):
        def step(i, c):
            dd, td = i >> 2, 4 * d + (i & 3)

            @pl.when(jnp.logical_not((dd == d) & (td == t)))
            def _():
                body(i, td, dd)

            return c

        lax.fori_loop(0, 32, step, 0)

    bar = pltpu.get_barrier_semaphore()

    def greet(td, dd):
        pl.semaphore_signal(bar, inc=1, device_id=dev(td, dd), device_id_type=MESH)

    for dd in range(8):
        for j in range(4):
            alone = jnp.logical_not(own & (d == dd) & (y == j))
            pl.when(alone)(functools.partial(greet, 4 * d + j, dd))
    for i in range(1, 8):
        greet(t, (d + i) & 7)

    fetch = [pltpu.make_async_copy(a, b, gsem.at[i]) for i, (a, b) in enumerate(zip(given, held))]
    for copy in fetch:
        copy.start()
    load = [pltpu.make_async_copy(state.at[l], st.at[l], lsem.at[l]) for l in range(2)]
    for l in range(2):
        load[l].start()
    fetch[0].wait()
    tile_x[...] = jnp.zeros((8, 128), BF16)
    tile_x[0:6, :] = tok[...]
    pl.semaphore_wait(bar, 39 - own.astype(jnp.int32))

    def tokens_out(i, c):
        td = far_first(i)

        @pl.when(jnp.logical_not(own & (td == t)))
        def _():
            send(tile_x, xbuf.at[4 * d + y], T0, td, z)

        return c

    lax.fori_loop(0, 32, tokens_out, 0)

    @pl.when(own)
    def _():
        xbuf[4 * d + y] = tile_x[...]

    for copy in fetch[1:]:
        copy.wait()
    for l in range(2):
        head = jnp.concatenate(
            [ww[l].astype(F32), wr[l].astype(F32), ws[0, l : l + 1, :].astype(F32), jnp.zeros((15, 128), F32)], axis=0
        )
        wst[l, 0:32, :] = head.astype(BF16)
        wst[l, 32:96, :] = wv[l]
        wst[l, 96:160, :] = wg[l]

    def first_weights(dd):
        send(ngain, gain.at[:, col], GAIN, t, dd)
        send(wst.at[0, 0:32], wfull.at[0, 0:32, col], INW0, t, dd)
        send(wst.at[1, 0:32], wfull.at[1, 0:32, col], INW1, t, dd)

    to_dp(first_weights)
    to_dp(lambda dd: send(wst.at[0, 32:160], wfull.at[0, 32:160, col], IN0, t, dd))
    to_dp(lambda dd: send(wo.at[0], wofull.at[0, :, col], OUT0, t, dd))
    to_dp(lambda dd: send(wst.at[1, 32:160], wfull.at[1, 32:160, col], IN1, t, dd))
    to_dp(lambda dd: send(wo.at[1], wofull.at[1, :, col], OUT1, t, dd))

    for l in range(2):
        wfull[l, :, col] = wst[l]
        wofull[l, :, col] = wo[l]
    gain[:, col] = ngain[...]
    srow = iota((24, 32), 0)
    six = (srow >= 6).astype(jnp.int32) + (srow >= 12).astype(jnp.int32) + (srow >= 18).astype(jnp.int32)
    place_b = (srow + 2 * six == iota((24, 32), 1)).astype(F32).astype(BF16)
    len_row = lengths[...].astype(F32)
    len_pad = jnp.dot(jnp.broadcast_to(len_row, (8, 24)).astype(BF16), place_b, preferred_element_type=F32)[0:1]
    len_col = as_column(len_row)
    for l in range(2):
        base_v = jnp.zeros((64, 32), F32)
        base_wr = jnp.zeros((16, 32), F32)
        for k in range(3):
            live_pad = (len_pad >= float(3 - k)).astype(F32)
            base_v += as_column(cv[l, k : k + 1, :]) * (dot(hv[l, k], place_b, 0, 0) * live_pad)
            base_w = as_column(cw[l, k : k + 1, :]) * (dot(hw[l, k], place_b, 1, 0) * live_pad)
            base_r = as_column(cr[l, k : k + 1, :]) * (dot(hr[l, k], place_b, 1, 0) * live_pad)
            base_wr += jnp.concatenate([base_w, base_r], axis=0)
            if k > 0:
                live_row = (len_row >= float(3 - k)).astype(F32)
                live_col = (len_col >= float(3 - k)).astype(F32)
                nhv[l, k - 1] = (hv[l, k].astype(F32) * live_col).astype(BF16)
                nhw[l, k - 1] = (hw[l, k].astype(F32) * live_row).astype(BF16)
                nhr[l, k - 1] = (hr[l, k].astype(F32) * live_row).astype(BF16)
        cbv[l] = base_v
        t3v[l] = jnp.broadcast_to(as_column(cv[l, 3:4, :]), (64, 32))
        tap_w = jnp.broadcast_to(as_column(cw[l, 3:4, :]), (8, 32))
        tap_r = jnp.broadcast_to(as_column(cr[l, 3:4, :]), (8, 32))
        if l == 0:
            cbwr[...] = base_wr
            t3wr[...] = jnp.concatenate([tap_w, tap_r], axis=0)
        else:
            cbsend[...] = jnp.concatenate([base_wr[0:8], base_wr[8:16], tap_w, tap_r], axis=1)
        ggc[l] = jnp.broadcast_to(as_column(gg[l : l + 1, :]), (64, 32))
    group = (t >= 16).astype(jnp.int32)
    sel_row = iota((256, 128), 0)
    for g in range(2):
        sel[g] = (((sel_row >> 1) == iota((256, 128), 1)) & ((sel_row & 1) == g)).astype(F32).astype(BF16)
    for l in range(2):
        load[l].wait()
        for s in range(24):
            stb[l, 64 * s : 64 * s + 64, :] = st[l, s].astype(BF16)

    wait_31_or_32(xbuf.at[0:31], xbuf, rsem.at[T0])
    wait(gain.at[:, 0:896], rsem.at[GAIN])

    lane = iota((64, 32), 1)
    sub8 = iota((8, 128), 0)
    lane8 = iota((8, 128), 1)
    for l in range(2):
        source = [xbuf[4 * a : 4 * a + 4] if l == 0 else agbuf[4 * a : 4 * a + 4, 0] for a in range(8)]
        xs = [x.astype(F32).reshape(32, 128) for x in source]
        squares = xs[0] * xs[0]
        for a in range(1, 8):
            squares += xs[a] * xs[a]
        scale = lax.rsqrt(jnp.sum(squares, axis=1, keepdims=True) / 1024.0 + EPS)
        normed = jnp.concatenate(
            [(xs[a] * scale * gain[l : l + 1, 128 * a : 128 * a + 128]).astype(BF16) for a in range(8)], axis=1
        )
        if l == 0:
            wait(wfull.at[0, 0:32, 0:896], rsem.at[INW0])
            first = dot(wfull[0, 0:32, :], normed, 1, 1)
            wr_new = first[0:16].astype(BF16)
            wr_act = silu(cbwr[...] + t3wr[...] * wr_new.astype(F32))
            wr_tile = jnp.concatenate([wr_act[0:8], wr_act[8:16], jnp.zeros((8, 64), F32)], axis=1).astype(BF16)
            wrsend[...] = wr_tile
            to_tp(lambda td: send(wrsend, wrbuf.at[t], WR0, td, d))
            wrbuf[t] = wr_tile
            wait(wfull.at[1, 0:32, 0:896], rsem.at[INW1])
            map_rows = wfull[1, 0:16, :].astype(F32)
            wpsend[0] = map_rows[0:8].astype(BF16)
            wpsend[1] = map_rows[8:16].astype(BF16)

            def piece_rows(td):
                return wpsend.at[:, :, pl.ds(pl.multiple_of((td >> 2) * 128, 128), 128)]

            to_tp(lambda td: send(piece_rows(td), wpbuf.at[:, t], WP, td, d))
            for m in range(2):
                wpbuf[m, t] = wpsend[m, :, pl.ds(pl.multiple_of(z * 128, 128), 128)]
            wait(wfull.at[0, 32:160, 0:896], rsem.at[IN0])
            rest = dot(wfull[0, 32:160, :], normed, 1, 1)
        else:
            wait(wfull.at[1, 32:160, 0:896], rsem.at[IN1])
            first = dot(wfull[1], normed, 1, 1)
            wr_new = first[0:16].astype(BF16)
            rest = first[32:160]
            maps = []
            for m in range(2):
                raw_map = agbuf[0:4, 1 + m].astype(F32)
                for a in range(1, 8):
                    raw_map += agbuf[4 * a : 4 * a + 4, 1 + m].astype(F32)
                new_map = (raw_map.reshape(32, 128) * scale).astype(BF16).astype(F32)
                maps.append(silu(conv_maps[32 * m : 32 * m + 32] + conv_maps[64 + 32 * m : 96 + 32 * m] * new_map))
            w_map, r_map = maps

        value_new = rest[0:64].astype(BF16)
        u = silu(cbv[l] + t3v[l] * value_new.astype(F32))
        gate = silu(rest[64:128].astype(BF16).astype(F32))
        raw = first[16:17] + sb[0:1, l : l + 1]
        step = jnp.maximum(raw, 0.0) + jnp.log1p(jnp.exp(-jnp.abs(raw)))
        keep = jnp.exp(-dr[0:1, l : l + 1] * step)
        su = u * step
        if l == 0:
            wait(wrbuf.at[0:31], rsem.at[WR0])
            maps = dot(wrbuf[...].reshape(256, 128), sel[group], 0, 0)
            w_map, r_map = maps[0:32], maps[32:64]
        r_b = r_map.astype(BF16)
        stored = dot(stb[l], r_b, 1, 1)
        readout = jnp.zeros((64, 32), F32)
        for s in range(24):
            p = s + 2 * (s // 6)
            readout = jnp.where(lane == p, stored[64 * s : 64 * s + 64], readout)
        wr_dot = as_row(jnp.sum(w_map * r_map, axis=1, keepdims=True))
        gated = (keep * readout + su * wr_dot + sg[0:1, l : l + 1] * u) * gate
        sq = jnp.sum(gated * gated, axis=0, keepdims=True)
        sq_hi = sq.astype(BF16).astype(F32)
        sq_lo = sq - sq_hi
        pad = jnp.zeros((1, 96), F32)
        row_hi = jnp.concatenate([sq_hi, pad], axis=1)
        row_lo = jnp.concatenate([sq_lo, pad], axis=1)
        mixer = (gated * ggc[l]).astype(BF16)
        wait(wofull.at[l, :, 0:896], rsem.at[OUT0 if l == 0 else OUT1])
        part = dot(mixer, wofull[l], 0, 0)
        for a in range(8):
            for k in range(4):
                piece = part[8 * k : 8 * k + 8, 128 * a : 128 * a + 128]
                piece = jnp.where(sub8 == 6, row_hi, jnp.where(sub8 == 7, row_lo, piece))
                rsend[l, 4 * a + k] = piece.astype(BF16)
        if l == 0:
            to_tp(lambda td: send(rsend.at[0, td], rbuf.at[0, t], RS0, td, d))
            rbuf[0, t] = rsend[0, t]
            to_tp(lambda td: send(cbsend, cbbuf.at[t], CB, td, d))
            cbbuf[t] = cbsend[...]
        else:
            to_across(lambda i, td, dd: send(rsend.at[1, i], rbuf.at[1, t], RS1, td, dd))

            @pl.when(own)
            def _():
                rbuf[1, t] = rsend[1, t]

        w_b = w_map.astype(BF16)
        keepb[...] = jnp.broadcast_to(as_column(keep), (32, 128))
        for s in range(24):
            p = s + 2 * (s // 6)
            outer = dot(jnp.where(lane == p, su, 0.0).astype(BF16), w_b, 1, 0)
            nstate[l, s] = keepb[p : p + 1, :] * st[l, s] + outer
        nhv[l, 2] = dot(place_b, value_new, 1, 1).astype(BF16)
        wr_nat = dot(wr_new, place_b, 1, 1)
        nhw[l, 2] = wr_nat[0:8].astype(BF16)
        nhr[l, 2] = wr_nat[8:16].astype(BF16)
        if l == 0:
            wait(wpbuf.at[:, 0:31], rsem.at[WP])
            for m in range(2):
                rows = wpbuf[m].reshape(256, 128)
                for g in range(2):
                    wperm[g, 128 * m : 128 * m + 128, :] = dot(sel[g], rows, 0, 0).astype(BF16)
            wait(rbuf.at[0, 0:31], rsem.at[RS0])
        else:
            wait_31_or_32(rbuf.at[1, 0:31], rbuf.at[1], rsem.at[RS1])

        total = jnp.zeros((8, 128), F32)
        for g in range(2):
            acc = jnp.sum(rbuf[l, 16 * g : 16 * g + 16].astype(F32), axis=0)
            sq_row = acc[6:7] + acc[7:8]
            sq_col = jnp.sum(
                jnp.where(lane8 == sub8 + 8 * y, jnp.broadcast_to(sq_row, (8, 128)), 0.0), axis=1, keepdims=True
            )
            total += acc * lax.rsqrt(sq_col / 1024.0 + EPS)
        if l == 0:
            tile = jnp.where(sub8 < 6, total, 0.0).astype(BF16)
            scaled = (tile.astype(F32) * gain[1:2, pl.ds(pl.multiple_of(z * 128, 128), 128)]).astype(BF16)
            for g in range(2):
                partial_maps = dot(scaled, wperm[g], 1, 1).astype(BF16)
                agsend[g, 0] = tile
                agsend[g, 1] = partial_maps[:, 0:128]
                agsend[g, 2] = partial_maps[:, 128:256]
            to_tp(lambda td: send(agsend.at[td >> 4], agbuf.at[t], AG0, td, d))
            agbuf[t] = agsend[group]
            wait(cbbuf.at[0:31], rsem.at[CB])
            conv_maps = lax.dot_general(
                cbbuf[...].reshape(256, 128), sel[group].astype(F32), (((0,), (0,)), ((), ())),
                precision=lax.Precision.HIGHEST, preferred_element_type=F32,
            )
            wait(agbuf.at[0:31], rsem.at[AG0])
        else:
            mixed[...] = total[0:6]

    wait_31_or_32(xbuf.at[0:31], xbuf, ssem.at[T0])
    wait_31_or_32(rbuf.at[1, 0:31], rbuf.at[1], ssem.at[RS1])
    wait(wpbuf.at[:, 0:31], ssem.at[WP])
    wait(gain.at[:, 0:896], ssem.at[GAIN])
    wait(wfull.at[0, 0:32, 0:896], ssem.at[INW0])
    wait(wfull.at[1, 0:32, 0:896], ssem.at[INW1])
    wait(wfull.at[0, 32:160, 0:896], ssem.at[IN0])
    wait(wfull.at[1, 32:160, 0:896], ssem.at[IN1])
    wait(wofull.at[0, :, 0:896], ssem.at[OUT0])
    wait(wofull.at[1, :, 0:896], ssem.at[OUT1])
    wait(wrbuf.at[0:31], ssem.at[WR0])
    wait(cbbuf.at[0:31], ssem.at[CB])
    wait(rbuf.at[0, 0:31], ssem.at[RS0])
    wait(agbuf.at[0:31], ssem.at[AG0])


def finish(*refs):
    given, outs, sem = refs[:5], refs[5:10], refs[10]
    copies = [pltpu.make_async_copy(a, b, sem.at[i]) for i, (a, b) in enumerate(zip(given, outs))]
    for copy in copies:
        copy.start()
    for copy in copies:
        copy.wait()


def local(
    tokens, lengths, norm_gain, w_gate, w_value, w_write, w_read, w_step, step_bias, decay_rate, skip_gain,
    conv_value_w, conv_write_w, conv_read_w, group_gain, w_out, state, hist_value, hist_write, hist_read,
):
    def flip(w):
        return jnp.transpose(w, (0, 2, 1))

    state = state.reshape(2, 24, 64, 128)
    args = (
        tokens, lengths.reshape(1, 24), norm_gain, flip(w_gate), flip(w_value), flip(w_write), flip(w_read),
        jnp.transpose(w_step, (2, 0, 1)), step_bias.T, decay_rate.T, skip_gain.T,
        conv_value_w, conv_write_w, conv_read_w, group_gain, w_out,
        jnp.transpose(hist_value, (0, 2, 1, 3)), jnp.transpose(hist_write, (0, 2, 3, 1)),
        jnp.transpose(hist_read, (0, 2, 3, 1)), state,
    )
    vmem = pl.BlockSpec(memory_space=pltpu.VMEM)
    hbm = pl.BlockSpec(memory_space=pl.ANY)
    outs = (
        ((6, 128), F32), ((2, 24, 64, 128), F32), ((2, 3, 24, 64), BF16), ((2, 3, 8, 24), BF16), ((2, 3, 8, 24), BF16),
    )
    held = pl.pallas_call(
        kernel,
        out_shape=tuple(pltpu.VMEM(*o) for o in outs),
        in_specs=[pl.BlockSpec(memory_space=pltpu.HBM)] * 20,
        out_specs=(vmem,) * 5,
        scratch_shapes=[
            *[pltpu.VMEM(a.shape, a.dtype) for a in args[:19]],
            pltpu.VMEM((8, 128), BF16),
            pltpu.VMEM((32, 8, 128), BF16),
            pltpu.VMEM((2, 160, 128), BF16),
            pltpu.VMEM((2, 160, 1024), BF16),
            pltpu.VMEM((2, 64, 1024), BF16),
            pltpu.VMEM((2, 1024), F32),
            pltpu.VMEM((2, 24, 64, 128), F32),
            pltpu.VMEM((2, 1536, 128), BF16),
            pltpu.VMEM((2, 256, 128), BF16),
            pltpu.VMEM((2, 64, 32), F32),
            pltpu.VMEM((2, 64, 32), F32),
            pltpu.VMEM((16, 32), F32),
            pltpu.VMEM((16, 32), F32),
            pltpu.VMEM((2, 64, 32), F32),
            pltpu.VMEM((8, 128), BF16),
            pltpu.VMEM((32, 8, 128), BF16),
            pltpu.VMEM((2, 32, 8, 128), BF16),
            pltpu.VMEM((2, 32, 8, 128), BF16),
            pltpu.VMEM((2, 3, 8, 128), BF16),
            pltpu.VMEM((32, 3, 8, 128), BF16),
            pltpu.VMEM((8, 128), F32),
            pltpu.VMEM((32, 8, 128), F32),
            pltpu.VMEM((2, 8, 1024), BF16),
            pltpu.VMEM((2, 32, 8, 128), BF16),
            pltpu.VMEM((2, 256, 128), BF16),
            pltpu.VMEM((32, 128), F32),
            pltpu.SemaphoreType.DMA((EXCHANGES,)),
            pltpu.SemaphoreType.DMA((EXCHANGES,)),
            pltpu.SemaphoreType.DMA((2,)),
            pltpu.SemaphoreType.DMA((19,)),
        ],
        compiler_params=pltpu.CompilerParams(collective_id=0, has_side_effects=True),
    )(*args)
    mixed, nstate, nhv, nhw, nhr = pl.pallas_call(
        finish,
        out_shape=tuple(jax.ShapeDtypeStruct(*o) for o in outs),
        in_specs=[vmem] * 5,
        out_specs=(hbm,) * 5,
        scratch_shapes=[pltpu.SemaphoreType.DMA((5,))],
    )(*(pltpu.with_memory_space_constraint(h, pltpu.VMEM) for h in held))
    return (
        mixed,
        nstate.reshape(2, 24, 1, 64, 128),
        jnp.transpose(nhv, (0, 2, 1, 3)),
        jnp.transpose(nhw, (0, 3, 1, 2)),
        jnp.transpose(nhr, (0, 3, 1, 2)),
    )


def solution(mesh):
    return jax.shard_map(
        local,
        mesh=mesh,
        in_specs=(
            P("tp", "dp"),
            P("dp"),
            P(None, "dp"),
            P(None, "dp", "tp"),
            P(None, "dp", "tp"),
            P(None, "dp", "tp"),
            P(None, "dp", "tp"),
            P(None, "dp", "tp"),
            P(None, "tp"),
            P(None, "tp"),
            P(None, "tp"),
            P(None, None, "tp"),
            P(None, None, "tp"),
            P(None, None, "tp"),
            P(None, "tp"),
            P(None, "tp", "dp"),
            P(None, "dp", "tp", None, None),
            P(None, "dp", None, "tp"),
            P(None, "dp", None, "tp"),
            P(None, "dp", None, "tp"),
        ),
        out_specs=(
            P("tp", "dp"),
            P(None, "dp", "tp", None, None),
            P(None, "dp", None, "tp"),
            P(None, "dp", None, "tp"),
            P(None, "dp", None, "tp"),
        ),
        check_vma=False,
    )
```

```python
import functools

import jax
import jax.numpy as jnp
from jax import lax
from jax.experimental import pallas as pl
from jax.experimental.pallas import tpu as pltpu
from jax.sharding import PartitionSpec as P

MESH = pl.DeviceIdType.MESH
F32 = jnp.float32
BF16 = jnp.bfloat16
EPS = 1e-05

T0, GAIN, INW0, INW1, IN0, IN1, OUT0, OUT1, WR0, CB, WP, RS0, AG0, PM0, RS1 = range(15)
EXCHANGES = 15


def iota(shape, dim):
    return lax.broadcasted_iota(jnp.int32, shape, dim)


def silu(x):
    return x / (1.0 + jnp.exp(-x))


def as_column(row):
    n = row.shape[1]
    square = jnp.broadcast_to(row, (n, n))
    return jnp.sum(jnp.where(iota((n, n), 0) == iota((n, n), 1), square, 0.0), axis=1, keepdims=True)


def as_row(column):
    n = column.shape[0]
    square = jnp.broadcast_to(column, (n, n))
    return jnp.sum(jnp.where(iota((n, n), 0) == iota((n, n), 1), square, 0.0), axis=0, keepdims=True)


def dot(a, b, ca, cb):
    return lax.dot_general(a, b, (((ca,), (cb,)), ((), ())), preferred_element_type=F32)


def kernel(*refs):
    given, state, outs, held, rest = refs[:19], refs[19], refs[20:25], refs[25:44], refs[44:]
    tok, lengths, ngain, wg, wv, ww, wr, ws, sb, dr, sg, cv, cw, cr, gg, wo, hv, hw, hr = held
    mixed, nstate, nhv, nhw, nhr = outs
    (
        tile_x, xbuf, wst, wfull, wofull, gain, st, stb, sel, cbv, t3v, cbwr, t3wr, ggc,
        wrsend, wrbuf, rsend, rbuf, agsend, agbuf, cbsend, cbbuf, wpsend, wpbuf, wperm, keepb,
        ssem, rsem, lsem, gsem,
    ) = rest
    t = lax.axis_index("tp")
    d = lax.axis_index("dp")
    z, y = t >> 2, t & 3
    own = z == d
    col = pl.ds(pl.multiple_of(d * 128, 128), 128)

    def dev(td, dd):
        return {"tp": td, "dp": dd}

    def send(src, dst, ex, td, dd):
        pltpu.make_async_remote_copy(
            src_ref=src, dst_ref=dst, send_sem=ssem.at[ex], recv_sem=rsem.at[ex],
            device_id=dev(td, dd), device_id_type=MESH,
        ).start()

    def wait(ref, sem):
        pltpu.make_async_copy(ref, ref, sem).wait()

    def wait_31_or_32(part, ref, sem):
        @pl.when(own)
        def _():
            wait(part, sem)

        @pl.when(jnp.logical_not(own))
        def _():
            wait(ref, sem)

    def far_first(i):
        q, p = i >> 2, i & 3
        dz = 4 + (1 - 2 * (q & 1)) * ((q + 1) >> 1)
        dy = 2 + (1 - 2 * (p & 1)) * ((p + 1) >> 1)
        return (((z + dz) & 7) << 2) + ((y + dy) & 3)

    def to_tp(body):
        def step(i, c):
            body(far_first(i))
            return c

        lax.fori_loop(0, 31, step, 0)

    def to_dp(body):
        def step(i, c):
            body((d + i) & 7)
            return c

        lax.fori_loop(1, 8, step, 0)

    def to_across(body):
        def step(i, c):
            dd, td = i >> 2, 4 * d + (i & 3)

            @pl.when(jnp.logical_not((dd == d) & (td == t)))
            def _():
                body(i, td, dd)

            return c

        lax.fori_loop(0, 32, step, 0)

    bar = pltpu.get_barrier_semaphore()

    def greet(td, dd):
        pl.semaphore_signal(bar, inc=1, device_id=dev(td, dd), device_id_type=MESH)

    for dd in range(8):
        for j in range(4):
            alone = jnp.logical_not(own & (d == dd) & (y == j))
            pl.when(alone)(functools.partial(greet, 4 * d + j, dd))
    for i in range(1, 8):
        greet(t, (d + i) & 7)

    fetch = [pltpu.make_async_copy(a, b, gsem.at[i]) for i, (a, b) in enumerate(zip(given, held))]
    for copy in fetch:
        copy.start()
    load = [pltpu.make_async_copy(state.at[l], st.at[l], lsem.at[l]) for l in range(2)]
    for l in range(2):
        load[l].start()
    fetch[0].wait()
    tile_x[...] = jnp.zeros((8, 128), BF16)
    tile_x[0:6, :] = tok[...]
    pl.semaphore_wait(bar, 39 - own.astype(jnp.int32))

    def tokens_out(i, c):
        td = far_first(i)

        @pl.when(jnp.logical_not(own & (td == t)))
        def _():
            send(tile_x, xbuf.at[4 * d + y], T0, td, z)

        return c

    lax.fori_loop(0, 32, tokens_out, 0)

    @pl.when(own)
    def _():
        xbuf[4 * d + y] = tile_x[...]

    for copy in fetch[1:]:
        copy.wait()
    for l in range(2):
        head = jnp.concatenate(
            [ww[l].astype(F32), wr[l].astype(F32), ws[0, l : l + 1, :].astype(F32), jnp.zeros((15, 128), F32)], axis=0
        )
        wst[l, 0:32, :] = head.astype(BF16)
        wst[l, 32:96, :] = wv[l]
        wst[l, 96:160, :] = wg[l]

    def first_weights(dd):
        send(ngain, gain.at[:, col], GAIN, t, dd)
        send(wst.at[0, 0:32], wfull.at[0, 0:32, col], INW0, t, dd)
        send(wst.at[1, 0:32], wfull.at[1, 0:32, col], INW1, t, dd)

    to_dp(first_weights)
    to_dp(lambda dd: send(wst.at[0, 32:160], wfull.at[0, 32:160, col], IN0, t, dd))
    to_dp(lambda dd: send(wo.at[0], wofull.at[0, :, col], OUT0, t, dd))
    to_dp(lambda dd: send(wst.at[1, 32:160], wfull.at[1, 32:160, col], IN1, t, dd))
    to_dp(lambda dd: send(wo.at[1], wofull.at[1, :, col], OUT1, t, dd))

    for l in range(2):
        wfull[l, :, col] = wst[l]
        wofull[l, :, col] = wo[l]
    gain[:, col] = ngain[...]
    srow = iota((24, 32), 0)
    six = (srow >= 6).astype(jnp.int32) + (srow >= 12).astype(jnp.int32) + (srow >= 18).astype(jnp.int32)
    place_b = (srow + 2 * six == iota((24, 32), 1)).astype(F32).astype(BF16)
    len_row = lengths[...].astype(F32)
    len_pad = jnp.dot(jnp.broadcast_to(len_row, (8, 24)).astype(BF16), place_b, preferred_element_type=F32)[0:1]
    len_col = as_column(len_row)
    for l in range(2):
        base_v = jnp.zeros((64, 32), F32)
        base_wr = jnp.zeros((16, 32), F32)
        for k in range(3):
            live_pad = (len_pad >= float(3 - k)).astype(F32)
            base_v += as_column(cv[l, k : k + 1, :]) * (dot(hv[l, k], place_b, 0, 0) * live_pad)
            base_w = as_column(cw[l, k : k + 1, :]) * (dot(hw[l, k], place_b, 1, 0) * live_pad)
            base_r = as_column(cr[l, k : k + 1, :]) * (dot(hr[l, k], place_b, 1, 0) * live_pad)
            base_wr += jnp.concatenate([base_w, base_r], axis=0)
            if k > 0:
                live_row = (len_row >= float(3 - k)).astype(F32)
                live_col = (len_col >= float(3 - k)).astype(F32)
                nhv[l, k - 1] = (hv[l, k].astype(F32) * live_col).astype(BF16)
                nhw[l, k - 1] = (hw[l, k].astype(F32) * live_row).astype(BF16)
                nhr[l, k - 1] = (hr[l, k].astype(F32) * live_row).astype(BF16)
        cbv[l] = base_v
        t3v[l] = jnp.broadcast_to(as_column(cv[l, 3:4, :]), (64, 32))
        tap_w = jnp.broadcast_to(as_column(cw[l, 3:4, :]), (8, 32))
        tap_r = jnp.broadcast_to(as_column(cr[l, 3:4, :]), (8, 32))
        if l == 0:
            cbwr[...] = base_wr
            t3wr[...] = jnp.concatenate([tap_w, tap_r], axis=0)
        else:
            cbsend[...] = jnp.concatenate([base_wr[0:8], base_wr[8:16], tap_w, tap_r], axis=1)
        ggc[l] = jnp.broadcast_to(as_column(gg[l : l + 1, :]), (64, 32))
    group = (t >= 16).astype(jnp.int32)
    sel_row = iota((256, 128), 0)
    for g in range(2):
        sel[g] = (((sel_row >> 1) == iota((256, 128), 1)) & ((sel_row & 1) == g)).astype(F32).astype(BF16)
    for l in range(2):
        load[l].wait()
        for s in range(24):
            stb[l, 64 * s : 64 * s + 64, :] = st[l, s].astype(BF16)

    wait_31_or_32(xbuf.at[0:31], xbuf, rsem.at[T0])
    wait(gain.at[:, 0:896], rsem.at[GAIN])

    lane = iota((64, 32), 1)
    sub8 = iota((8, 128), 0)
    lane8 = iota((8, 128), 1)
    for l in range(2):
        source = [xbuf[4 * a : 4 * a + 4] if l == 0 else agbuf[4 * a : 4 * a + 4, 0] for a in range(8)]
        xs = [x.astype(F32).reshape(32, 128) for x in source]
        squares = xs[0] * xs[0]
        for a in range(1, 8):
            squares += xs[a] * xs[a]
        scale = lax.rsqrt(jnp.sum(squares, axis=1, keepdims=True) / 1024.0 + EPS)
        normed = jnp.concatenate(
            [(xs[a] * scale * gain[l : l + 1, 128 * a : 128 * a + 128]).astype(BF16) for a in range(8)], axis=1
        )
        if l == 0:
            wait(wfull.at[0, 0:32, 0:896], rsem.at[INW0])
            first = dot(wfull[0, 0:32, :], normed, 1, 1)
            wr_new = first[0:16].astype(BF16)
            wr_act = silu(cbwr[...] + t3wr[...] * wr_new.astype(F32))
            wr_tile = jnp.concatenate([wr_act[0:8], wr_act[8:16], jnp.zeros((8, 64), F32)], axis=1).astype(BF16)
            wrsend[...] = wr_tile
            to_tp(lambda td: send(wrsend, wrbuf.at[t], WR0, td, d))
            wrbuf[t] = wr_tile
            wait(wfull.at[1, 0:32, 0:896], rsem.at[INW1])
            map_rows = wfull[1, 0:16, :].astype(F32)
            wpsend[0] = map_rows[0:8].astype(BF16)
            wpsend[1] = map_rows[8:16].astype(BF16)

            def piece_rows(td):
                return wpsend.at[:, :, pl.ds(pl.multiple_of((td >> 2) * 128, 128), 128)]

            to_tp(lambda td: send(piece_rows(td), wpbuf.at[:, t], WP, td, d))
            for m in range(2):
                wpbuf[m, t] = wpsend[m, :, pl.ds(pl.multiple_of(z * 128, 128), 128)]
            wait(wfull.at[0, 32:160, 0:896], rsem.at[IN0])
            rest = dot(wfull[0, 32:160, :], normed, 1, 1)
        else:
            wait(wfull.at[1, 32:160, 0:896], rsem.at[IN1])
            first = dot(wfull[1], normed, 1, 1)
            wr_new = first[0:16].astype(BF16)
            rest = first[32:160]
        value_new = rest[0:64].astype(BF16)
        u = silu(cbv[l] + t3v[l] * value_new.astype(F32))
        gate = silu(rest[64:128].astype(BF16).astype(F32))
        raw = first[16:17] + sb[0:1, l : l + 1]
        step = jnp.maximum(raw, 0.0) + jnp.log1p(jnp.exp(-jnp.abs(raw)))
        keep = jnp.exp(-dr[0:1, l : l + 1] * step)
        su = u * step
        if l == 0:
            wait(wrbuf.at[0:31], rsem.at[WR0])
            maps = dot(wrbuf[...].reshape(256, 128), sel[group], 0, 0)
            w_map, r_map = maps[0:32], maps[32:64]
        else:
            wait(agbuf.at[0:31, 1:3], rsem.at[PM0])
            maps = []
            for m in range(2):
                raw_map = agbuf[0:4, 1 + m].astype(F32)
                for a in range(1, 8):
                    raw_map += agbuf[4 * a : 4 * a + 4, 1 + m].astype(F32)
                new_map = (raw_map.reshape(32, 128) * scale).astype(BF16).astype(F32)
                maps.append(silu(conv_maps[32 * m : 32 * m + 32] + conv_maps[64 + 32 * m : 96 + 32 * m] * new_map))
            w_map, r_map = maps
        r_b = r_map.astype(BF16)
        stored = dot(stb[l], r_b, 1, 1)
        readout = jnp.zeros((64, 32), F32)
        for s in range(24):
            p = s + 2 * (s // 6)
            readout = jnp.where(lane == p, stored[64 * s : 64 * s + 64], readout)
        wr_dot = as_row(jnp.sum(w_map * r_map, axis=1, keepdims=True))
        gated = (keep * readout + su * wr_dot + sg[0:1, l : l + 1] * u) * gate
        sq = jnp.sum(gated * gated, axis=0, keepdims=True)
        sq_hi = sq.astype(BF16).astype(F32)
        sq_lo = sq - sq_hi
        pad = jnp.zeros((1, 96), F32)
        row_hi = jnp.concatenate([sq_hi, pad], axis=1)
        row_lo = jnp.concatenate([sq_lo, pad], axis=1)
        mixer = (gated * ggc[l]).astype(BF16)
        wait(wofull.at[l, :, 0:896], rsem.at[OUT0 if l == 0 else OUT1])
        part = dot(mixer, wofull[l], 0, 0)
        for a in range(8):
            for k in range(4):
                piece = part[8 * k : 8 * k + 8, 128 * a : 128 * a + 128]
                piece = jnp.where(sub8 == 6, row_hi, jnp.where(sub8 == 7, row_lo, piece))
                rsend[l, 4 * a + k] = piece.astype(BF16)
        if l == 0:
            to_tp(lambda td: send(rsend.at[0, td], rbuf.at[0, t], RS0, td, d))
            rbuf[0, t] = rsend[0, t]
            to_tp(lambda td: send(cbsend, cbbuf.at[t], CB, td, d))
            cbbuf[t] = cbsend[...]
        else:
            to_across(lambda i, td, dd: send(rsend.at[1, i], rbuf.at[1, t], RS1, td, dd))

            @pl.when(own)
            def _():
                rbuf[1, t] = rsend[1, t]

        w_b = w_map.astype(BF16)
        keepb[...] = jnp.broadcast_to(as_column(keep), (32, 128))
        for s in range(24):
            p = s + 2 * (s // 6)
            outer = dot(jnp.where(lane == p, su, 0.0).astype(BF16), w_b, 1, 0)
            nstate[l, s] = keepb[p : p + 1, :] * st[l, s] + outer
        nhv[l, 2] = dot(place_b, value_new, 1, 1).astype(BF16)
        wr_nat = dot(wr_new, place_b, 1, 1)
        nhw[l, 2] = wr_nat[0:8].astype(BF16)
        nhr[l, 2] = wr_nat[8:16].astype(BF16)
        if l == 0:
            wait(wpbuf.at[:, 0:31], rsem.at[WP])
            for m in range(2):
                rows = wpbuf[m].reshape(256, 128)
                for g in range(2):
                    wperm[g, 128 * m : 128 * m + 128, :] = dot(sel[g], rows, 0, 0).astype(BF16)
            wait(rbuf.at[0, 0:31], rsem.at[RS0])
        else:
            wait_31_or_32(rbuf.at[1, 0:31], rbuf.at[1], rsem.at[RS1])

        total = jnp.zeros((8, 128), F32)
        for g in range(2):
            acc = jnp.sum(rbuf[l, 16 * g : 16 * g + 16].astype(F32), axis=0)
            sq_row = acc[6:7] + acc[7:8]
            sq_col = jnp.sum(
                jnp.where(lane8 == sub8 + 8 * y, jnp.broadcast_to(sq_row, (8, 128)), 0.0), axis=1, keepdims=True
            )
            total += acc * lax.rsqrt(sq_col / 1024.0 + EPS)
        if l == 0:
            tile = jnp.where(sub8 < 6, total, 0.0).astype(BF16)
            agsend[0, 0] = tile
            to_tp(lambda td: send(agsend.at[0, 0], agbuf.at[t, 0], AG0, td, d))
            scaled = (tile.astype(F32) * gain[1:2, pl.ds(pl.multiple_of(z * 128, 128), 128)]).astype(BF16)
            for g in range(2):
                partial_maps = dot(scaled, wperm[g], 1, 1).astype(BF16)
                agsend[g, 1] = partial_maps[:, 0:128]
                agsend[g, 2] = partial_maps[:, 128:256]
            to_tp(lambda td: send(agsend.at[td >> 4, 1:3], agbuf.at[t, 1:3], PM0, td, d))
            agbuf[t, 0] = tile
            agbuf[t, 1:3] = agsend[group, 1:3]
            wait(cbbuf.at[0:31], rsem.at[CB])
            conv_maps = lax.dot_general(
                cbbuf[...].reshape(256, 128), sel[group].astype(F32), (((0,), (0,)), ((), ())),
                precision=lax.Precision.HIGHEST, preferred_element_type=F32,
            )
            wait(agbuf.at[0:31, 0], rsem.at[AG0])
        else:
            mixed[...] = total[0:6]

    wait_31_or_32(xbuf.at[0:31], xbuf, ssem.at[T0])
    wait_31_or_32(rbuf.at[1, 0:31], rbuf.at[1], ssem.at[RS1])
    wait(wpbuf.at[:, 0:31], ssem.at[WP])
    wait(gain.at[:, 0:896], ssem.at[GAIN])
    wait(wfull.at[0, 0:32, 0:896], ssem.at[INW0])
    wait(wfull.at[1, 0:32, 0:896], ssem.at[INW1])
    wait(wfull.at[0, 32:160, 0:896], ssem.at[IN0])
    wait(wfull.at[1, 32:160, 0:896], ssem.at[IN1])
    wait(wofull.at[0, :, 0:896], ssem.at[OUT0])
    wait(wofull.at[1, :, 0:896], ssem.at[OUT1])
    wait(wrbuf.at[0:31], ssem.at[WR0])
    wait(cbbuf.at[0:31], ssem.at[CB])
    wait(rbuf.at[0, 0:31], ssem.at[RS0])
    wait(agbuf.at[0:31, 0], ssem.at[AG0])
    wait(agbuf.at[0:31, 1:3], ssem.at[PM0])


def finish(*refs):
    given, outs, sem = refs[:5], refs[5:10], refs[10]
    copies = [pltpu.make_async_copy(a, b, sem.at[i]) for i, (a, b) in enumerate(zip(given, outs))]
    for copy in copies:
        copy.start()
    for copy in copies:
        copy.wait()


def local(
    tokens, lengths, norm_gain, w_gate, w_value, w_write, w_read, w_step, step_bias, decay_rate, skip_gain,
    conv_value_w, conv_write_w, conv_read_w, group_gain, w_out, state, hist_value, hist_write, hist_read,
):
    def flip(w):
        return jnp.transpose(w, (0, 2, 1))

    state = state.reshape(2, 24, 64, 128)
    args = (
        tokens, lengths.reshape(1, 24), norm_gain, flip(w_gate), flip(w_value), flip(w_write), flip(w_read),
        jnp.transpose(w_step, (2, 0, 1)), step_bias.T, decay_rate.T, skip_gain.T,
        conv_value_w, conv_write_w, conv_read_w, group_gain, w_out,
        jnp.transpose(hist_value, (0, 2, 1, 3)), jnp.transpose(hist_write, (0, 2, 3, 1)),
        jnp.transpose(hist_read, (0, 2, 3, 1)), state,
    )
    vmem = pl.BlockSpec(memory_space=pltpu.VMEM)
    hbm = pl.BlockSpec(memory_space=pl.ANY)
    outs = (
        ((6, 128), F32), ((2, 24, 64, 128), F32), ((2, 3, 24, 64), BF16), ((2, 3, 8, 24), BF16), ((2, 3, 8, 24), BF16),
    )
    held = pl.pallas_call(
        kernel,
        out_shape=tuple(pltpu.VMEM(*o) for o in outs),
        in_specs=[pl.BlockSpec(memory_space=pltpu.HBM)] * 20,
        out_specs=(vmem,) * 5,
        scratch_shapes=[
            *[pltpu.VMEM(a.shape, a.dtype) for a in args[:19]],
            pltpu.VMEM((8, 128), BF16),
            pltpu.VMEM((32, 8, 128), BF16),
            pltpu.VMEM((2, 160, 128), BF16),
            pltpu.VMEM((2, 160, 1024), BF16),
            pltpu.VMEM((2, 64, 1024), BF16),
            pltpu.VMEM((2, 1024), F32),
            pltpu.VMEM((2, 24, 64, 128), F32),
            pltpu.VMEM((2, 1536, 128), BF16),
            pltpu.VMEM((2, 256, 128), BF16),
            pltpu.VMEM((2, 64, 32), F32),
            pltpu.VMEM((2, 64, 32), F32),
            pltpu.VMEM((16, 32), F32),
            pltpu.VMEM((16, 32), F32),
            pltpu.VMEM((2, 64, 32), F32),
            pltpu.VMEM((8, 128), BF16),
            pltpu.VMEM((32, 8, 128), BF16),
            pltpu.VMEM((2, 32, 8, 128), BF16),
            pltpu.VMEM((2, 32, 8, 128), BF16),
            pltpu.VMEM((2, 3, 8, 128), BF16),
            pltpu.VMEM((32, 3, 8, 128), BF16),
            pltpu.VMEM((8, 128), F32),
            pltpu.VMEM((32, 8, 128), F32),
            pltpu.VMEM((2, 8, 1024), BF16),
            pltpu.VMEM((2, 32, 8, 128), BF16),
            pltpu.VMEM((2, 256, 128), BF16),
            pltpu.VMEM((32, 128), F32),
            pltpu.SemaphoreType.DMA((EXCHANGES,)),
            pltpu.SemaphoreType.DMA((EXCHANGES,)),
            pltpu.SemaphoreType.DMA((2,)),
            pltpu.SemaphoreType.DMA((19,)),
        ],
        compiler_params=pltpu.CompilerParams(collective_id=0, has_side_effects=True),
    )(*args)
    mixed, nstate, nhv, nhw, nhr = pl.pallas_call(
        finish,
        out_shape=tuple(jax.ShapeDtypeStruct(*o) for o in outs),
        in_specs=[vmem] * 5,
        out_specs=(hbm,) * 5,
        scratch_shapes=[pltpu.SemaphoreType.DMA((5,))],
    )(*(pltpu.with_memory_space_constraint(h, pltpu.VMEM) for h in held))
    return (
        mixed,
        nstate.reshape(2, 24, 1, 64, 128),
        jnp.transpose(nhv, (0, 2, 1, 3)),
        jnp.transpose(nhw, (0, 3, 1, 2)),
        jnp.transpose(nhr, (0, 3, 1, 2)),
    )


def solution(mesh):
    return jax.shard_map(
        local,
        mesh=mesh,
        in_specs=(
            P("tp", "dp"),
            P("dp"),
            P(None, "dp"),
            P(None, "dp", "tp"),
            P(None, "dp", "tp"),
            P(None, "dp", "tp"),
            P(None, "dp", "tp"),
            P(None, "dp", "tp"),
            P(None, "tp"),
            P(None, "tp"),
            P(None, "tp"),
            P(None, None, "tp"),
            P(None, None, "tp"),
            P(None, None, "tp"),
            P(None, "tp"),
            P(None, "tp", "dp"),
            P(None, "dp", "tp", None, None),
            P(None, "dp", None, "tp"),
            P(None, "dp", None, "tp"),
            P(None, "dp", None, "tp"),
        ),
        out_specs=(
            P("tp", "dp"),
            P(None, "dp", "tp", None, None),
            P(None, "dp", None, "tp"),
            P(None, "dp", None, "tp"),
            P(None, "dp", None, "tp"),
        ),
        check_vma=False,
    )
```

```python
import functools

import jax
import jax.numpy as jnp
from jax import lax
from jax.experimental import pallas as pl
from jax.experimental.pallas import tpu as pltpu
from jax.sharding import PartitionSpec as P

MESH = pl.DeviceIdType.MESH
F32 = jnp.float32
BF16 = jnp.bfloat16
EPS = 1e-05

T0, GAIN, INW0, INW1, IN0, IN1, OUT0, OUT1, WR0, CB, WP, RS0, AG0, PM0, RS1 = range(15)
EXCHANGES = 15


def iota(shape, dim):
    return lax.broadcasted_iota(jnp.int32, shape, dim)


def silu(x):
    return x / (1.0 + jnp.exp(-x))


def as_column(row):
    n = row.shape[1]
    square = jnp.broadcast_to(row, (n, n))
    return jnp.sum(jnp.where(iota((n, n), 0) == iota((n, n), 1), square, 0.0), axis=1, keepdims=True)


def as_row(column):
    n = column.shape[0]
    square = jnp.broadcast_to(column, (n, n))
    return jnp.sum(jnp.where(iota((n, n), 0) == iota((n, n), 1), square, 0.0), axis=0, keepdims=True)


def dot(a, b, ca, cb):
    return lax.dot_general(a, b, (((ca,), (cb,)), ((), ())), preferred_element_type=F32)


def kernel(*refs):
    given, state, outs, held, rest = refs[:19], refs[19], refs[20:25], refs[25:44], refs[44:]
    tok, lengths, ngain, wg, wv, ww, wr, ws, sb, dr, sg, cv, cw, cr, gg, wo, hv, hw, hr = held
    mixed, nstate, nhv, nhw, nhr = outs
    (
        tile_x, xbuf, wst, wfull, wofull, gain, st, stb, sel, cbv, t3v, cbwr, t3wr, ggc,
        wrsend, wrbuf, rsend, rbuf, agsend, agbuf, cbsend, cbbuf, wpsend, wpbuf, wperm, keepb,
        ssem, rsem, lsem, gsem,
    ) = rest
    t = lax.axis_index("tp")
    d = lax.axis_index("dp")
    z, y = t >> 2, t & 3
    own = z == d
    col = pl.ds(pl.multiple_of(d * 128, 128), 128)

    def dev(td, dd):
        return {"tp": td, "dp": dd}

    def send(src, dst, ex, td, dd):
        pltpu.make_async_remote_copy(
            src_ref=src, dst_ref=dst, send_sem=ssem.at[ex], recv_sem=rsem.at[ex],
            device_id=dev(td, dd), device_id_type=MESH,
        ).start()

    def wait(ref, sem):
        pltpu.make_async_copy(ref, ref, sem).wait()

    def wait_31_or_32(part, ref, sem):
        @pl.when(own)
        def _():
            wait(part, sem)

        @pl.when(jnp.logical_not(own))
        def _():
            wait(ref, sem)

    def far_first(i):
        q, p = i >> 2, i & 3
        dz = 4 + (1 - 2 * (q & 1)) * ((q + 1) >> 1)
        dy = 2 + (1 - 2 * (p & 1)) * ((p + 1) >> 1)
        return (((z + dz) & 7) << 2) + ((y + dy) & 3)

    def to_tp(body):
        def step(i, c):
            body(far_first(i))
            return c

        lax.fori_loop(0, 31, step, 0)

    def to_dp(body):
        def step(i, c):
            body((d + i) & 7)
            return c

        lax.fori_loop(1, 8, step, 0)

    def to_across(body):
        def step(i, c):
            dd, td = i >> 2, 4 * d + (i & 3)

            @pl.when(jnp.logical_not((dd == d) & (td == t)))
            def _():
                body(i, td, dd)

            return c

        lax.fori_loop(0, 32, step, 0)

    bar = pltpu.get_barrier_semaphore()

    def greet(td, dd):
        pl.semaphore_signal(bar, inc=1, device_id=dev(td, dd), device_id_type=MESH)

    for dd in range(8):
        for j in range(4):
            alone = jnp.logical_not(own & (d == dd) & (y == j))
            pl.when(alone)(functools.partial(greet, 4 * d + j, dd))
    for i in range(1, 8):
        greet(t, (d + i) & 7)

    fetch = [pltpu.make_async_copy(a, b, gsem.at[i]) for i, (a, b) in enumerate(zip(given, held))]
    for copy in fetch:
        copy.start()
    load = [pltpu.make_async_copy(state.at[l], st.at[l], lsem.at[l]) for l in range(2)]
    for l in range(2):
        load[l].start()
    fetch[0].wait()
    tile_x[...] = jnp.zeros((8, 128), BF16)
    tile_x[0:6, :] = tok[...]
    pl.semaphore_wait(bar, 39 - own.astype(jnp.int32))

    def tokens_out(i, c):
        td = far_first(i)

        @pl.when(jnp.logical_not(own & (td == t)))
        def _():
            send(tile_x, xbuf.at[4 * d + y], T0, td, z)

        return c

    lax.fori_loop(0, 32, tokens_out, 0)

    @pl.when(own)
    def _():
        xbuf[4 * d + y] = tile_x[...]

    for copy in fetch[1:]:
        copy.wait()
    for l in range(2):
        head = jnp.concatenate(
            [ww[l].astype(F32), wr[l].astype(F32), ws[0, l : l + 1, :].astype(F32), jnp.zeros((15, 128), F32)], axis=0
        )
        wst[l, 0:32, :] = head.astype(BF16)
        wst[l, 32:96, :] = wv[l]
        wst[l, 96:160, :] = wg[l]

    def first_weights(dd):
        send(ngain, gain.at[:, col], GAIN, t, dd)
        send(wst.at[0, 0:32], wfull.at[0, 0:32, col], INW0, t, dd)
        send(wst.at[1, 0:32], wfull.at[1, 0:32, col], INW1, t, dd)

    to_dp(first_weights)
    to_dp(lambda dd: send(wst.at[0, 32:160], wfull.at[0, 32:160, col], IN0, t, dd))
    to_dp(lambda dd: send(wo.at[0], wofull.at[0, :, col], OUT0, t, dd))
    to_dp(lambda dd: send(wst.at[1, 32:160], wfull.at[1, 32:160, col], IN1, t, dd))
    to_dp(lambda dd: send(wo.at[1], wofull.at[1, :, col], OUT1, t, dd))

    for l in range(2):
        wfull[l, :, col] = wst[l]
        wofull[l, :, col] = wo[l]
    gain[:, col] = ngain[...]
    srow = iota((24, 32), 0)
    six = (srow >= 6).astype(jnp.int32) + (srow >= 12).astype(jnp.int32) + (srow >= 18).astype(jnp.int32)
    place_b = (srow + 2 * six == iota((24, 32), 1)).astype(F32).astype(BF16)
    len_row = lengths[...].astype(F32)
    len_pad = jnp.dot(jnp.broadcast_to(len_row, (8, 24)).astype(BF16), place_b, preferred_element_type=F32)[0:1]
    len_col = as_column(len_row)
    for l in range(2):
        base_v = jnp.zeros((64, 32), F32)
        base_wr = jnp.zeros((16, 32), F32)
        for k in range(3):
            live_pad = (len_pad >= float(3 - k)).astype(F32)
            base_v += as_column(cv[l, k : k + 1, :]) * (dot(hv[l, k], place_b, 0, 0) * live_pad)
            base_w = as_column(cw[l, k : k + 1, :]) * (dot(hw[l, k], place_b, 1, 0) * live_pad)
            base_r = as_column(cr[l, k : k + 1, :]) * (dot(hr[l, k], place_b, 1, 0) * live_pad)
            base_wr += jnp.concatenate([base_w, base_r], axis=0)
            if k > 0:
                live_row = (len_row >= float(3 - k)).astype(F32)
                live_col = (len_col >= float(3 - k)).astype(F32)
                nhv[l, k - 1] = (hv[l, k].astype(F32) * live_col).astype(BF16)
                nhw[l, k - 1] = (hw[l, k].astype(F32) * live_row).astype(BF16)
                nhr[l, k - 1] = (hr[l, k].astype(F32) * live_row).astype(BF16)
        cbv[l] = base_v
        t3v[l] = jnp.broadcast_to(as_column(cv[l, 3:4, :]), (64, 32))
        tap_w = jnp.broadcast_to(as_column(cw[l, 3:4, :]), (8, 32))
        tap_r = jnp.broadcast_to(as_column(cr[l, 3:4, :]), (8, 32))
        if l == 0:
            cbwr[...] = base_wr
            t3wr[...] = jnp.concatenate([tap_w, tap_r], axis=0)
        else:
            cbsend[...] = jnp.concatenate([base_wr[0:8], base_wr[8:16], tap_w, tap_r], axis=1)
        ggc[l] = jnp.broadcast_to(as_column(gg[l : l + 1, :]), (64, 32))
    group = (t >= 16).astype(jnp.int32)
    sel_row = iota((256, 128), 0)
    for g in range(2):
        sel[g] = (((sel_row >> 1) == iota((256, 128), 1)) & ((sel_row & 1) == g)).astype(F32).astype(BF16)
    for l in range(2):
        load[l].wait()
        for s in range(24):
            stb[l, 64 * s : 64 * s + 64, :] = st[l, s].astype(BF16)

    wait_31_or_32(xbuf.at[0:31], xbuf, rsem.at[T0])
    wait(gain.at[:, 0:896], rsem.at[GAIN])

    lane = iota((64, 32), 1)
    sub8 = iota((8, 128), 0)
    lane8 = iota((8, 128), 1)
    for l in range(2):
        source = [xbuf[4 * a : 4 * a + 4] if l == 0 else agbuf[4 * a : 4 * a + 4, 0] for a in range(8)]
        xs = [x.astype(F32).reshape(32, 128) for x in source]
        squares = xs[0] * xs[0]
        for a in range(1, 8):
            squares += xs[a] * xs[a]
        scale = lax.rsqrt(jnp.sum(squares, axis=1, keepdims=True) / 1024.0 + EPS)
        normed = jnp.concatenate(
            [(xs[a] * scale * gain[l : l + 1, 128 * a : 128 * a + 128]).astype(BF16) for a in range(8)], axis=1
        )
        if l == 0:
            wait(wfull.at[0, 0:32, 0:896], rsem.at[INW0])
            first = dot(wfull[0, 0:32, :], normed, 1, 1)
            wr_new = first[0:16].astype(BF16)
            wr_act = silu(cbwr[...] + t3wr[...] * wr_new.astype(F32))
            wr_tile = jnp.concatenate([wr_act[0:8], wr_act[8:16], jnp.zeros((8, 64), F32)], axis=1).astype(BF16)
            wrsend[...] = wr_tile
            to_tp(lambda td: send(wrsend, wrbuf.at[t], WR0, td, d))
            wrbuf[t] = wr_tile
            wait(wfull.at[1, 0:32, 0:896], rsem.at[INW1])
            map_rows = wfull[1, 0:16, :].astype(F32)
            wpsend[0] = map_rows[0:8].astype(BF16)
            wpsend[1] = map_rows[8:16].astype(BF16)

            def piece_rows(td):
                return wpsend.at[:, :, pl.ds(pl.multiple_of((td >> 2) * 128, 128), 128)]

            to_tp(lambda td: send(piece_rows(td), wpbuf.at[:, t], WP, td, d))
            for m in range(2):
                wpbuf[m, t] = wpsend[m, :, pl.ds(pl.multiple_of(z * 128, 128), 128)]
            wait(wfull.at[0, 32:160, 0:896], rsem.at[IN0])
            rest = dot(wfull[0, 32:160, :], normed, 1, 1)
        else:
            wait(wfull.at[1, 32:160, 0:896], rsem.at[IN1])
            first = dot(wfull[1], normed, 1, 1)
            wr_new = first[0:16].astype(BF16)
            rest = first[32:160]
        value_new = rest[0:64].astype(BF16)
        u = silu(cbv[l] + t3v[l] * value_new.astype(F32))
        gate = silu(rest[64:128].astype(BF16).astype(F32))
        raw = first[16:17] + sb[0:1, l : l + 1]
        step = jnp.maximum(raw, 0.0) + jnp.log1p(jnp.exp(-jnp.abs(raw)))
        keep = jnp.exp(-dr[0:1, l : l + 1] * step)
        su = u * step
        if l == 0:
            wait(wrbuf.at[0:31], rsem.at[WR0])
            maps = dot(wrbuf[...].reshape(256, 128), sel[group], 0, 0)
            w_map, r_map = maps[0:32], maps[32:64]
        else:
            wait(agbuf.at[0:31, 1:3], rsem.at[PM0])
            maps = []
            for m in range(2):
                raw_map = agbuf[0:4, 1 + m].astype(F32)
                for a in range(1, 8):
                    raw_map += agbuf[4 * a : 4 * a + 4, 1 + m].astype(F32)
                new_map = (raw_map.reshape(32, 128) * scale).astype(BF16).astype(F32)
                maps.append(silu(conv_maps[32 * m : 32 * m + 32] + conv_maps[64 + 32 * m : 96 + 32 * m] * new_map))
            w_map, r_map = maps
        r_b = r_map.astype(BF16)
        stored = dot(stb[l], r_b, 1, 1)
        readout = jnp.zeros((64, 32), F32)
        for s in range(24):
            p = s + 2 * (s // 6)
            readout = jnp.where(lane == p, stored[64 * s : 64 * s + 64], readout)
        wr_dot = as_row(jnp.sum(w_map * r_map, axis=1, keepdims=True))
        gated = (keep * readout + su * wr_dot + sg[0:1, l : l + 1] * u) * gate
        sq = jnp.sum(gated * gated, axis=0, keepdims=True)
        sq_hi = sq.astype(BF16).astype(F32)
        sq_lo = sq - sq_hi
        pad = jnp.zeros((1, 96), F32)
        row_hi = jnp.concatenate([sq_hi, pad], axis=1)
        row_lo = jnp.concatenate([sq_lo, pad], axis=1)
        mixer = (gated * ggc[l]).astype(BF16)
        wait(wofull.at[l, :, 0:896], rsem.at[OUT0 if l == 0 else OUT1])
        part = dot(mixer, wofull[l], 0, 0)
        for a in range(8):
            for k in range(4):
                piece = part[8 * k : 8 * k + 8, 128 * a : 128 * a + 128]
                piece = jnp.where(sub8 == 6, row_hi, jnp.where(sub8 == 7, row_lo, piece))
                rsend[l, 4 * a + k] = piece.astype(BF16)
        if l == 0:
            to_tp(lambda td: send(rsend.at[0, td], rbuf.at[0, t], RS0, td, d))
            rbuf[0, t] = rsend[0, t]
            to_tp(lambda td: send(cbsend, cbbuf.at[t], CB, td, d))
            cbbuf[t] = cbsend[...]
        else:

            def parts(i, c):
                dd, k = (d + 4 + 2 * (i & 3) + ((i >> 2) & 1)) & 7, (i >> 3) & 3
                td = 4 * d + k

                @pl.when(jnp.logical_not((dd == d) & (td == t)))
                def _():
                    send(rsend.at[1, 4 * dd + k], rbuf.at[1, t], RS1, td, dd)

                return c

            lax.fori_loop(0, 32, parts, 0)

            @pl.when(own)
            def _():
                rbuf[1, t] = rsend[1, t]

        w_b = w_map.astype(BF16)
        keepb[...] = jnp.broadcast_to(as_column(keep), (32, 128))
        for s in range(24):
            p = s + 2 * (s // 6)
            outer = dot(jnp.where(lane == p, su, 0.0).astype(BF16), w_b, 1, 0)
            nstate[l, s] = keepb[p : p + 1, :] * st[l, s] + outer
        nhv[l, 2] = dot(place_b, value_new, 1, 1).astype(BF16)
        wr_nat = dot(wr_new, place_b, 1, 1)
        nhw[l, 2] = wr_nat[0:8].astype(BF16)
        nhr[l, 2] = wr_nat[8:16].astype(BF16)
        if l == 0:
            wait(wpbuf.at[:, 0:31], rsem.at[WP])
            for m in range(2):
                rows = wpbuf[m].reshape(256, 128)
                for g in range(2):
                    wperm[g, 128 * m : 128 * m + 128, :] = dot(sel[g], rows, 0, 0).astype(BF16)
            wait(rbuf.at[0, 0:31], rsem.at[RS0])
        else:
            wait_31_or_32(rbuf.at[1, 0:31], rbuf.at[1], rsem.at[RS1])

        total = jnp.zeros((8, 128), F32)
        for g in range(2):
            acc = jnp.sum(rbuf[l, 16 * g : 16 * g + 16].astype(F32), axis=0)
            sq_row = acc[6:7] + acc[7:8]
            sq_col = jnp.sum(
                jnp.where(lane8 == sub8 + 8 * y, jnp.broadcast_to(sq_row, (8, 128)), 0.0), axis=1, keepdims=True
            )
            total += acc * lax.rsqrt(sq_col / 1024.0 + EPS)
        if l == 0:
            tile = jnp.where(sub8 < 6, total, 0.0).astype(BF16)
            agsend[0, 0] = tile
            to_tp(lambda td: send(agsend.at[0, 0], agbuf.at[t, 0], AG0, td, d))
            scaled = (tile.astype(F32) * gain[1:2, pl.ds(pl.multiple_of(z * 128, 128), 128)]).astype(BF16)
            for g in range(2):
                partial_maps = dot(scaled, wperm[g], 1, 1).astype(BF16)
                agsend[g, 1] = partial_maps[:, 0:128]
                agsend[g, 2] = partial_maps[:, 128:256]
            to_tp(lambda td: send(agsend.at[td >> 4, 1:3], agbuf.at[t, 1:3], PM0, td, d))
            agbuf[t, 0] = tile
            agbuf[t, 1:3] = agsend[group, 1:3]
            wait(cbbuf.at[0:31], rsem.at[CB])
            conv_maps = lax.dot_general(
                cbbuf[...].reshape(256, 128), sel[group].astype(F32), (((0,), (0,)), ((), ())),
                precision=lax.Precision.HIGHEST, preferred_element_type=F32,
            )
            wait(agbuf.at[0:31, 0], rsem.at[AG0])
        else:
            mixed[...] = total[0:6]

    wait_31_or_32(xbuf.at[0:31], xbuf, ssem.at[T0])
    wait_31_or_32(rbuf.at[1, 0:31], rbuf.at[1], ssem.at[RS1])
    wait(wpbuf.at[:, 0:31], ssem.at[WP])
    wait(gain.at[:, 0:896], ssem.at[GAIN])
    wait(wfull.at[0, 0:32, 0:896], ssem.at[INW0])
    wait(wfull.at[1, 0:32, 0:896], ssem.at[INW1])
    wait(wfull.at[0, 32:160, 0:896], ssem.at[IN0])
    wait(wfull.at[1, 32:160, 0:896], ssem.at[IN1])
    wait(wofull.at[0, :, 0:896], ssem.at[OUT0])
    wait(wofull.at[1, :, 0:896], ssem.at[OUT1])
    wait(wrbuf.at[0:31], ssem.at[WR0])
    wait(cbbuf.at[0:31], ssem.at[CB])
    wait(rbuf.at[0, 0:31], ssem.at[RS0])
    wait(agbuf.at[0:31, 0], ssem.at[AG0])
    wait(agbuf.at[0:31, 1:3], ssem.at[PM0])


def finish(*refs):
    given, outs, sem = refs[:5], refs[5:10], refs[10]
    copies = [pltpu.make_async_copy(a, b, sem.at[i]) for i, (a, b) in enumerate(zip(given, outs))]
    for copy in copies:
        copy.start()
    for copy in copies:
        copy.wait()


def local(
    tokens, lengths, norm_gain, w_gate, w_value, w_write, w_read, w_step, step_bias, decay_rate, skip_gain,
    conv_value_w, conv_write_w, conv_read_w, group_gain, w_out, state, hist_value, hist_write, hist_read,
):
    def flip(w):
        return jnp.transpose(w, (0, 2, 1))

    state = state.reshape(2, 24, 64, 128)
    args = (
        tokens, lengths.reshape(1, 24), norm_gain, flip(w_gate), flip(w_value), flip(w_write), flip(w_read),
        jnp.transpose(w_step, (2, 0, 1)), step_bias.T, decay_rate.T, skip_gain.T,
        conv_value_w, conv_write_w, conv_read_w, group_gain, w_out,
        jnp.transpose(hist_value, (0, 2, 1, 3)), jnp.transpose(hist_write, (0, 2, 3, 1)),
        jnp.transpose(hist_read, (0, 2, 3, 1)), state,
    )
    vmem = pl.BlockSpec(memory_space=pltpu.VMEM)
    hbm = pl.BlockSpec(memory_space=pl.ANY)
    outs = (
        ((6, 128), F32), ((2, 24, 64, 128), F32), ((2, 3, 24, 64), BF16), ((2, 3, 8, 24), BF16), ((2, 3, 8, 24), BF16),
    )
    held = pl.pallas_call(
        kernel,
        out_shape=tuple(pltpu.VMEM(*o) for o in outs),
        in_specs=[pl.BlockSpec(memory_space=pltpu.HBM)] * 20,
        out_specs=(vmem,) * 5,
        scratch_shapes=[
            *[pltpu.VMEM(a.shape, a.dtype) for a in args[:19]],
            pltpu.VMEM((8, 128), BF16),
            pltpu.VMEM((32, 8, 128), BF16),
            pltpu.VMEM((2, 160, 128), BF16),
            pltpu.VMEM((2, 160, 1024), BF16),
            pltpu.VMEM((2, 64, 1024), BF16),
            pltpu.VMEM((2, 1024), F32),
            pltpu.VMEM((2, 24, 64, 128), F32),
            pltpu.VMEM((2, 1536, 128), BF16),
            pltpu.VMEM((2, 256, 128), BF16),
            pltpu.VMEM((2, 64, 32), F32),
            pltpu.VMEM((2, 64, 32), F32),
            pltpu.VMEM((16, 32), F32),
            pltpu.VMEM((16, 32), F32),
            pltpu.VMEM((2, 64, 32), F32),
            pltpu.VMEM((8, 128), BF16),
            pltpu.VMEM((32, 8, 128), BF16),
            pltpu.VMEM((2, 32, 8, 128), BF16),
            pltpu.VMEM((2, 32, 8, 128), BF16),
            pltpu.VMEM((2, 3, 8, 128), BF16),
            pltpu.VMEM((32, 3, 8, 128), BF16),
            pltpu.VMEM((8, 128), F32),
            pltpu.VMEM((32, 8, 128), F32),
            pltpu.VMEM((2, 8, 1024), BF16),
            pltpu.VMEM((2, 32, 8, 128), BF16),
            pltpu.VMEM((2, 256, 128), BF16),
            pltpu.VMEM((32, 128), F32),
            pltpu.SemaphoreType.DMA((EXCHANGES,)),
            pltpu.SemaphoreType.DMA((EXCHANGES,)),
            pltpu.SemaphoreType.DMA((2,)),
            pltpu.SemaphoreType.DMA((19,)),
        ],
        compiler_params=pltpu.CompilerParams(collective_id=0, has_side_effects=True),
    )(*args)
    mixed, nstate, nhv, nhw, nhr = pl.pallas_call(
        finish,
        out_shape=tuple(jax.ShapeDtypeStruct(*o) for o in outs),
        in_specs=[vmem] * 5,
        out_specs=(hbm,) * 5,
        scratch_shapes=[pltpu.SemaphoreType.DMA((5,))],
    )(*(pltpu.with_memory_space_constraint(h, pltpu.VMEM) for h in held))
    return (
        mixed,
        nstate.reshape(2, 24, 1, 64, 128),
        jnp.transpose(nhv, (0, 2, 1, 3)),
        jnp.transpose(nhw, (0, 3, 1, 2)),
        jnp.transpose(nhr, (0, 3, 1, 2)),
    )


def solution(mesh):
    return jax.shard_map(
        local,
        mesh=mesh,
        in_specs=(
            P("tp", "dp"),
            P("dp"),
            P(None, "dp"),
            P(None, "dp", "tp"),
            P(None, "dp", "tp"),
            P(None, "dp", "tp"),
            P(None, "dp", "tp"),
            P(None, "dp", "tp"),
            P(None, "tp"),
            P(None, "tp"),
            P(None, "tp"),
            P(None, None, "tp"),
            P(None, None, "tp"),
            P(None, None, "tp"),
            P(None, "tp"),
            P(None, "tp", "dp"),
            P(None, "dp", "tp", None, None),
            P(None, "dp", None, "tp"),
            P(None, "dp", None, "tp"),
            P(None, "dp", None, "tp"),
        ),
        out_specs=(
            P("tp", "dp"),
            P(None, "dp", "tp", None, None),
            P(None, "dp", None, "tp"),
            P(None, "dp", None, "tp"),
            P(None, "dp", None, "tp"),
        ),
        check_vma=False,
    )
```
